32 devices in a mesh: fs: 8 (over z, x), tp: 4 (over y, core).
Axes of the slice: x: 2, y: 2, z: 4, core: 2. Of those that a mesh axis runs over, the one named last changes fastest.
Arguments:
- x_late: bfloat16 [3072, 2048], P(('fs', 'tp')), may hold values from -6 to 6
- x_early: bfloat16 [3072, 2048], P(('fs', 'tp')), may hold values from -6 to 6
- cotangent: bfloat16 [3072, 2048], P(('fs', 'tp')), may hold values from -6 to 6
- up_weight: bfloat16 [2048, 4096], P('fs', 'tp'), may hold values from -0.125 to 0.125
- down_weight: bfloat16 [2048, 4096], P('fs', 'tp'), may hold values from -0.09375 to 0.09375
- up_grad_sum: float32 [2048, 4096], P('fs', 'tp'), may hold values from -24 to 24
- down_grad_sum: float32 [2048, 4096], P('fs', 'tp'), may hold values from -24 to 24
Outputs:
- output: bfloat16 [3072, 2048], P(('fs', 'tp'))
- input_grad: bfloat16 [3072, 2048], P(('fs', 'tp'))
- up_grad_new: float32 [2048, 4096], P('fs', 'tp')
- down_grad_new: float32 [2048, 4096], P('fs', 'tp')
The draws below stay inside these ranges and needn't reach their ends.
All inputs are finite; a program needn't handle non-finite values.
Results may differ from the reference program's by a relative error of at most 0.0095.
Values may be sent and summed in bfloat16 or wider, within the bound.
A program may use at most 128 MiB of HBM per device.

```python
import jax
import jax.numpy as jnp
from jax import lax

D = 2048
FF = 4096
TOKENS = 3072
N_TP = 4


def raised(result, rng, source, target, shards_of, factor):
    owner, partner = [(jnp.arange(result.shape[axis_at]) // (result.shape[axis_at] // shards_of)).reshape([-1 if axis == axis_at else 1 for axis in range(result.ndim)]) for axis_at in (source, target)]
    chosen = jax.random.permutation(rng, shards_of)[partner]
    strong = (owner == chosen) | (owner == (partner + shards_of // 2) % shards_of)
    return jnp.where(strong, factor * result, result)


def block_levels(stream_key, extent, split, low, top_value):
    def one(position, shards_of):
        draws = jax.random.uniform(jax.random.fold_in(jax.random.fold_in(stream_key, 6), position), (shards_of,), jnp.float32, low / len(split), top_value / len(split))
        return jnp.repeat(jnp.exp(draws), extent[position] // shards_of).reshape((-1,) + (1,) * (len(extent) - position - 1))

    level = one(*split[0])
    for cut in split[1:]:
        level = level * one(*cut)
    return level


def normal_values(stream_key, dims, scale, limit, cuts=(), dtype=jnp.bfloat16):
    entries = jax.random.normal(stream_key, dims, jnp.float32) * scale
    if len(cuts) > 0:
        entries = block_levels(stream_key, dims, cuts, -0.22, 0.18) * entries
    return jnp.clip(entries, min=-limit, max=limit).astype(dtype)


def noise_with(own_key, extent, deviation, reach, pieces, heavy, dtype=jnp.bfloat16):
    drawn = deviation * jax.random.normal(own_key, extent, jnp.float32)
    if pieces:
        drawn = drawn * block_levels(own_key, extent, pieces, -0.22, 0.18)
    return jnp.clip(raised(drawn, jax.random.fold_in(own_key, 3), *heavy), -reach, reach).astype(dtype)


def setup_inputs(seed: int = 0) -> dict:
    arg_keys = jax.random.split(jax.random.key(seed), 8)
    x_late = normal_values(arg_keys[0], (TOKENS, D), 1.0, 6.0, ((0, 32),))
    x_early = normal_values(arg_keys[1], (TOKENS, D), 1.0, 6.0, ((0, 32),))
    cotangent = noise_with(arg_keys[2], (TOKENS, D), 0.25, 6.0, ((0, 32),), (0, 1, 32, 2.75))
    up_weight = normal_values(arg_keys[3], (D, FF), D ** -0.5, 0.125, ((0, 8), (1, 4)))
    down_weight = normal_values(arg_keys[4], (D, FF), FF ** -0.5, 0.09375, ((0, 8), (1, 4)))
    up_grad_sum = normal_values(arg_keys[5], (D, FF), 4.0, 24.0, ((0, 8), (1, 4)), jnp.float32)
    down_grad_sum = normal_values(arg_keys[6], (D, FF), 4.0, 24.0, ((0, 8), (1, 4)), jnp.float32)
    return dict(x_late=x_late, x_early=x_early, cotangent=cotangent, up_weight=up_weight, down_weight=down_weight, up_grad_sum=up_grad_sum, down_grad_sum=down_grad_sum)


def dot_last(left, right):
    return lax.dot_general(left, right, (((1,), (1,)), ((), ())), preferred_element_type=jnp.float32)


def dot_first(left, right):
    return lax.dot_general(left, right, (((0,), (0,)), ((), ())), preferred_element_type=jnp.float32)


def tp_rounded(left, right):
    stride = right.shape[1] // N_TP
    totals = jnp.zeros((left.shape[0], right.shape[0]), jnp.float32)
    for column_block in range(N_TP):
        first_col = column_block * stride
        partial_value = dot_last(left[:, first_col:first_col + stride], right[:, first_col:first_col + stride])
        rounded = lax.optimization_barrier(partial_value.astype(jnp.bfloat16))
        totals = totals + rounded.astype(jnp.float32)
    return totals.astype(jnp.bfloat16)


def reference(x_late, x_early, cotangent, up_weight, down_weight, up_grad_sum, down_grad_sum):
    pre_late = jnp.dot(x_late, up_weight, preferred_element_type=jnp.float32)
    act_late = jnp.square(jax.nn.relu(pre_late)).astype(jnp.bfloat16)
    output = tp_rounded(act_late, down_weight)
    pre_early = jnp.dot(x_early, up_weight, preferred_element_type=jnp.float32)
    act_early = jnp.square(jax.nn.relu(pre_early)).astype(jnp.bfloat16)
    grad_act = jnp.dot(cotangent, down_weight, preferred_element_type=jnp.float32)
    grad_pre = (grad_act * 2.0 * jax.nn.relu(pre_early)).astype(jnp.bfloat16)
    input_grad = tp_rounded(grad_pre, up_weight)
    up_grad_new = up_grad_sum + dot_first(x_early, grad_pre)
    down_grad_new = down_grad_sum + dot_first(cotangent, act_early)
    return (output, input_grad, up_grad_new, down_grad_new)
```

```python
import functools

import jax
import jax.numpy as jnp
from jax import lax
from jax.experimental import pallas as pl
from jax.experimental.pallas import tpu as pltpu
from jax.sharding import PartitionSpec as P


MESH = pl.DeviceIdType.MESH
VMEM = pl.BlockSpec(memory_space=pltpu.VMEM)
EARLY, COT, LATE = 0, 1, 2
UP, DOWN = 0, 1
CHUNKS = 2


def dot(left, right, left_dim, right_dim):
    return lax.dot_general(
        left, right, (((left_dim,), (right_dim,)), ((), ())), preferred_element_type=jnp.float32
    )


def remote(src, dst, send, recv, fs, tp):
    return pltpu.make_async_remote_copy(
        src_ref=src, dst_ref=dst, send_sem=send, recv_sem=recv,
        device_id={"fs": fs, "tp": tp}, device_id_type=MESH,
    )


def layer_kernel(n_fo, n_tp, *refs):
    tokens, weights = refs[0:3], refs[3:5]
    summed, grads = refs[5:7], refs[7:9]
    (tok, wts, g_out, g_in, pre, hid, partial, landed, pair_sum, arrived, staged, other,
     local, t_send, t_recv, a_send, a_recv, zg_send, zg_recv,
     c_send, c_recv, p_send, p_recv, zr_send, zr_recv, x_send, x_recv) = refs[9:]
    fs, tp = lax.axis_index("fs"), lax.axis_index("tp")
    fo, fi = fs // 2, fs % 2
    y, core = tp // 2, tp % 2
    pair = fo * 2 + 1 - fi
    across_y = (1 - y) * 2 + core
    sibling = y * 2 + 1 - core
    rows, width = tokens[0].shape
    w_rows, cols = weights[0].shape
    half = cols // 2
    wide = half // CHUNKS
    count = 4 * rows * 2
    cut = rows // 96 * 16
    first, last = fo == 0, fo == n_fo - 1

    def side(part):
        return 1 - fi if part else fi

    def open_way(way):
        return jnp.logical_not(last) if way == 0 else jnp.logical_not(first)

    def ahead(way):
        return (fo + 1 - 2 * way) * 2 + fi

    spots = [(0, 0), (1, 0), (0, 1), (1, 1)]

    def slot(a, k, at_core):
        dx, dy = spots[k]
        return tok.at[a, (1 - fi if dx else fi), (1 - y if dy else y), at_core]

    def token(a, j):
        sems = t_send.at[a, j], t_recv.at[a, j]
        if j == 0:
            return remote(tokens[a], slot(a, 0, core), *sems, pair, tp)
        if j == 1:
            return remote(tokens[a], slot(a, 0, core), *sems, fs, across_y)
        if j == 2:
            part = slot(a, 2, core).at[pl.ds(0, cut)]
            return remote(part, part, *sems, pair, tp)
        if j == 3:
            part = slot(a, 1, core).at[pl.ds(cut, rows - cut)]
            return remote(part, part, *sems, fs, across_y)
        k = j - 4
        dst = slot(a, k, core)
        return remote(tokens[a] if k == 0 else dst, dst, *sems, fs, sibling)

    def token_in(a, j):
        sems = t_send.at[a, j], t_recv.at[a, j]
        if j < 2:
            dst = slot(a, 1 + j, core)
        elif j == 2:
            dst = slot(a, 3, core).at[pl.ds(0, cut)]
        elif j == 3:
            dst = slot(a, 3, core).at[pl.ds(cut, rows - cut)]
        else:
            dst = slot(a, j - 4, 1 - core)
        return remote(dst, dst, *sems, fs, sibling)

    def from_y(a):
        token_in(a, 1).wait_recv()
        token(a, 2).start()
        token(a, 6).start()

    def from_x(a):
        token_in(a, 0).wait_recv()
        token(a, 3).start()
        token(a, 5).start()

    def diagonal(a):
        token_in(a, 3).wait_recv()
        token_in(a, 2).wait_recv()
        token(a, 7).start()

    def from_sibling(a):
        for k in range(4):
            token_in(a, 4 + k).wait_recv()

    def columns(w, which, c):
        return weights[w].at[:, pl.ds(pl.multiple_of(which * half + c * wide, wide), wide)]

    def across(w, c):
        return remote(columns(w, 1 - fi, c), wts.at[w, c, fo, fi], a_send.at[w, c], a_recv.at[w, c], pair, tp)

    def across_in(w, c):
        dst = wts.at[w, c, fo, 1 - fi]
        return remote(dst, dst, a_send.at[w, c], a_recv.at[w, c], pair, tp)

    def along(w, c, source, part, way, src=None):
        dst = wts.at[w, c, source, side(part)]
        return remote(dst if src is None else src, dst, zg_send.at[way, w, c, source, part],
                      zg_recv.at[w, c, source, part], ahead(way), tp)

    def begin(c, way):
        for w in range(2):
            along(w, c, fo, 0, way, columns(w, fi, c)).start()

    def begin_after(c, distance):
        for way in range(2):
            @pl.when(open_way(way) & ((fo if way == 0 else n_fo - 1 - fo) == distance))
            def _():
                begin(c, way)

    def crossed(c):
        for w in range(2):
            across_in(w, c).wait_recv()
            for way in range(2):
                @pl.when(open_way(way))
                def _():
                    along(w, c, fo, 1, way).start()

    def incoming(way, distance):
        source = fo - distance if way == 0 else fo + distance
        return source, (source >= 0) & (source < n_fo)

    def forward(c, part, distance):
        for w in range(2):
            for way in range(2):
                source, inside = incoming(way, distance)

                @pl.when(inside & open_way(way))
                def _():
                    along(w, c, source, part, way).wait_recv()
                    along(w, c, source, part, way).start()

    def settle(c):
        for part in range(2):
            for distance in range(1, n_fo):
                for w in range(2):
                    for way in range(2):
                        source, inside = incoming(way, distance)

                        @pl.when(inside & jnp.logical_not(open_way(way)))
                        def _():
                            along(w, c, source, part, way).wait_recv()

    def flat(a):
        return tok[a].reshape(count, width)

    def weight(w, c):
        return wts[w, c].reshape(width, wide)

    def activate(c):
        relu = jnp.maximum(dot(flat(EARLY), weight(UP, c), 1, 0), 0.0)
        pre[...] = relu
        hid[0, c] = (relu * relu).astype(jnp.bfloat16)

    def hidden_grad(c):
        grad_act = dot(flat(COT), weight(DOWN, c), 1, 0)
        hid[1, c] = (grad_act * 2.0 * pre[...]).astype(jnp.bfloat16)

    def activate_late(c):
        relu = jnp.maximum(dot(flat(LATE), weight(UP, c), 1, 0), 0.0)
        hid[2, c] = (relu * relu).astype(jnp.bfloat16)

    n_half = n_fo // 2
    d_half = width // 2

    def weight_grad(w, c, step):
        at = jnp.where(fo < n_half, 1 - step, step)
        lanes = pl.ds(pl.multiple_of(at * d_half, d_half), d_half)
        left = tok[EARLY if w == UP else COT, :, :, :, :, lanes].reshape(count, d_half)
        value = dot(left, hid[1 if w == UP else 0, c], 0, 0)
        g_out[w, c, pl.ds(at * n_half, n_half)] = value.astype(jnp.bfloat16).reshape(n_half, 2, w_rows, wide)
        for k in range(n_half):
            for part in (1, 0):
                for way in range(2):
                    block = farthest(way, step, k)

                    @pl.when((first if way == 0 else last) & (fo != block))
                    def _():
                        grad(w, c, block, part, way, g_out.at[w, c, block, side(part)]).start()

    def token_partial(a, h, w):
        sources = max(1, 512 // (2 * w_rows))
        lanes = sources * 2 * w_rows
        for b in range(n_fo // sources):
            total = None
            for c in range(CHUNKS):
                right = wts[w, c, b * sources:(b + 1) * sources].reshape(lanes, wide)
                term = dot(hid[h, c], right, 1, 1)
                total = term if total is None else total + term
            partial[a, :, :, :, :, b * lanes:(b + 1) * lanes] = (
                total.astype(jnp.bfloat16).reshape(2, 2, 2, rows, lanes))
        near(a).start()

    def farthest(way, step, k):
        return n_fo - 1 - step * n_half - k if way == 0 else step * n_half + k

    def grad(w, c, block, part, way, src=None):
        held = g_in.at[way, w, c, block, part]
        return remote(held if src is None else src, held, zr_send.at[way, w, c, block, part],
                      zr_recv.at[way, w, c, block, part], ahead(way), tp)

    def carry(w, c, step, k):
        for part in (1, 0):
            for way in range(2):
                block = farthest(way, step, k)
                inside = (fo < block) & (fo > 0) if way == 0 else (fo > block) & (fo < n_fo - 1)

                @pl.when(inside)
                def _():
                    grad(w, c, block, part, way).wait_recv()
                    g_in[way, w, c, block, part] = (
                        g_out[w, c, block, side(part)].astype(jnp.float32)
                        + g_in[way, w, c, block, part].astype(jnp.float32)
                    ).astype(jnp.bfloat16)
                    grad(w, c, block, part, way).start()

    def carry_all(c):
        for step in range(2):
            for w in (DOWN, UP):
                for k in range(n_half):
                    carry(w, c, step, k)

    def swap(w, c):
        return remote(staged.at[w, c], other.at[w, c], x_send.at[w, c], x_recv.at[w, c], pair, tp)

    def owned(w, c, part):
        for way in range(2):
            @pl.when(first if way == 0 else last)
            def _():
                g_in[way, w, c, fo, part] = jnp.zeros(g_in.shape[5:], g_in.dtype)

            @pl.when(jnp.logical_not(first if way == 0 else last))
            def _():
                grad(w, c, fo, part, way).wait_recv()
        total = (g_out[w, c, fo, side(part)].astype(jnp.float32)
                 + g_in[0, w, c, fo, part].astype(jnp.float32)
                 + g_in[1, w, c, fo, part].astype(jnp.float32))
        if part:
            staged[w, c] = total.astype(jnp.bfloat16)
            swap(w, c).start()
        else:
            grads[w][:, pl.ds(pl.multiple_of(fi * half + c * wide, wide), wide)] = total

    def swapped(w, c):
        swap(w, c).wait_recv()
        grads[w][:, pl.ds(pl.multiple_of((1 - fi) * half + c * wide, wide), wide)] = (
            other[w, c].astype(jnp.float32))

    def spot(k):
        dx, dy = spots[k]
        return (1 - fi if dx else fi), (1 - y if dy else y)

    def near(a):
        return remote(partial.at[a, :, :, 1 - core], landed.at[a], c_send.at[a], c_recv.at[a], fs, sibling)

    def far(a, k):
        at_fi, at_y = spot(k)
        return remote(pair_sum.at[a, at_fi, at_y], arrived.at[a, k - 1], p_send.at[a, k], p_recv.at[a, k],
                      fo * 2 + at_fi, at_y * 2 + core)

    def joined(a, at_fi, at_y):
        return (partial[a, at_fi, at_y, core].astype(jnp.float32)
                + landed[a, at_fi, at_y].astype(jnp.float32))

    def spread(a):
        near(a).wait_recv()
        for k in (3, 1, 2):
            at_fi, at_y = spot(k)
            pair_sum[a, at_fi, at_y] = joined(a, at_fi, at_y).astype(jnp.bfloat16)
            far(a, k).start()

    def collect(a):
        total = joined(a, fi, y)
        for k in (1, 2, 3):
            far(a, k).wait_recv()
            total += arrived[a, k - 1].astype(jnp.float32)
        summed[a][...] = total.astype(jnp.bfloat16)

    barrier = pltpu.get_barrier_semaphore()

    def greet(to_fs, to_tp):
        pl.semaphore_signal(barrier, inc=1, device_id={"fs": to_fs, "tp": to_tp}, device_id_type=MESH)

    greet(pair, tp)
    greet(fs, across_y)
    greet(fs, sibling)
    greet(pair, across_y)
    for way in range(2):
        @pl.when(open_way(way))
        def _():
            greet(ahead(way), tp)
    pl.semaphore_wait(barrier, 4 + (fo > 0).astype(jnp.int32) + (fo < n_fo - 1).astype(jnp.int32))

    for way in range(2):
        @pl.when(open_way(way))
        def _():
            begin(0, way)
    for w in range(2):
        across(w, 0).start()
    for a in (EARLY, COT):
        token(a, 0).start()
        token(a, 1).start()
    for w in range(2):
        across(w, 1).start()
    for a in (EARLY, COT, LATE):
        token(a, 4).start()
    own = [pltpu.make_async_copy(tokens[a], slot(a, 0, core), local.at[a]) for a in range(3)]
    own += [pltpu.make_async_copy(columns(w, fi, c), wts.at[w, c, fo, fi], local.at[3 + w * CHUNKS + c])
            for w in range(2) for c in range(CHUNKS)]
    for copy in own:
        copy.start()

    inner = range(2, n_fo - 1)
    forward(0, 0, 1)
    crossed(0)
    begin_after(1, 0)
    from_y(EARLY)
    for distance in inner:
        forward(0, 0, distance)
    from_x(EARLY)
    forward(0, 1, 1)
    begin_after(1, 1)
    from_y(COT)
    for distance in inner:
        forward(0, 1, distance)
        begin_after(1, distance)
    from_x(COT)
    token(LATE, 0).start()
    token(LATE, 1).start()
    diagonal(EARLY)
    forward(1, 0, 1)
    crossed(1)
    diagonal(COT)
    for copy in own:
        copy.wait()
    from_sibling(EARLY)
    from_sibling(COT)
    settle(0)

    activate(0)
    weight_grad(DOWN, 0, 0)
    for distance in inner:
        forward(1, 0, distance)
    hidden_grad(0)
    weight_grad(UP, 0, 0)
    forward(1, 1, 1)
    weight_grad(DOWN, 0, 1)
    weight_grad(UP, 0, 1)
    from_y(LATE)
    from_x(LATE)
    for k in range(n_half):
        carry(DOWN, 0, 0, k)
        if k == 0:
            for distance in inner:
                forward(1, 1, distance)
            diagonal(LATE)
    from_sibling(LATE)
    activate_late(0)
    for k in range(n_half):
        carry(UP, 0, 0, k)
    for w in (DOWN, UP):
        for k in range(n_half):
            carry(w, 0, 1, k)

    settle(1)
    activate(1)
    weight_grad(DOWN, 1, 0)
    hidden_grad(1)
    weight_grad(UP, 1, 0)
    weight_grad(DOWN, 1, 1)
    weight_grad(UP, 1, 1)
    token_partial(1, 1, UP)
    activate_late(1)
    spread(1)
    token_partial(0, 2, DOWN)
    for k in range(n_half):
        carry(DOWN, 1, 0, k)
        if k == 0:
            spread(0)
            for w in (DOWN, UP):
                owned(w, 0, 1)
    for k in range(n_half):
        carry(UP, 1, 0, k)
    for w in (DOWN, UP):
        for k in range(n_half):
            carry(w, 1, 1, k)
    for w in (DOWN, UP):
        owned(w, 0, 0)
    for w in (DOWN, UP):
        swapped(w, 0)
    owned(DOWN, 1, 1)
    owned(DOWN, 1, 0)
    collect(1)
    owned(UP, 1, 1)
    owned(UP, 1, 0)
    collect(0)
    for w in (DOWN, UP):
        swapped(w, 1)

    for a in range(3):
        for j in range(8):
            token(a, j).wait_send()
    for w in range(2):
        for c in range(CHUNKS):
            across(w, c).wait_send()
            swap(w, c).wait_send()
            for way in range(2):
                @pl.when(open_way(way))
                def _():
                    for part in range(2):
                        along(w, c, fo, part, way).wait_send()

                for distance in range(1, n_fo):
                    source, inside = incoming(way, distance)

                    @pl.when(inside & open_way(way))
                    def _():
                        for part in range(2):
                            along(w, c, source, part, way).wait_send()

                for block in range(n_fo):
                    @pl.when(fo < block if way == 0 else fo > block)
                    def _():
                        for part in range(2):
                            grad(w, c, block, part, way).wait_send()
    for a in range(2):
        near(a).wait_send()
        for k in (1, 2, 3):
            far(a, k).wait_send()


def layer(n_fo, n_tp, tokens, weights):
    rows, width = tokens[0].shape
    w_rows, cols = weights[0].shape
    wide = cols // 2 // CHUNKS
    count = 8 * rows
    dma = pltpu.SemaphoreType.DMA
    bf16, f32 = jnp.bfloat16, jnp.float32
    return pl.pallas_call(
        functools.partial(layer_kernel, n_fo, n_tp),
        out_shape=[jax.ShapeDtypeStruct((rows, width), bf16)] * 2
        + [jax.ShapeDtypeStruct((w_rows, cols), f32)] * 2,
        in_specs=[VMEM] * 5,
        out_specs=[VMEM] * 4,
        scratch_shapes=[
            pltpu.VMEM((3, 2, 2, 2, rows, width), bf16),
            pltpu.VMEM((2, CHUNKS, n_fo, 2, w_rows, wide), bf16),
            pltpu.VMEM((2, CHUNKS, n_fo, 2, w_rows, wide), bf16),
            pltpu.VMEM((2, 2, CHUNKS, n_fo, 2, w_rows, wide), bf16),
            pltpu.VMEM((count, wide), f32),
            pltpu.VMEM((3, CHUNKS, count, wide), bf16),
            pltpu.VMEM((2, 2, 2, 2, rows, width), bf16),
            pltpu.VMEM((2, 2, 2, rows, width), bf16),
            pltpu.VMEM((2, 2, 2, rows, width), bf16),
            pltpu.VMEM((2, 3, rows, width), bf16),
            pltpu.VMEM((2, CHUNKS, w_rows, wide), bf16),
            pltpu.VMEM((2, CHUNKS, w_rows, wide), bf16),
            dma((3 + 2 * CHUNKS,)), dma((3, 8)), dma((3, 8)), dma((2, CHUNKS)), dma((2, CHUNKS)),
            dma((2, 2, CHUNKS, n_fo, 2)), dma((2, CHUNKS, n_fo, 2)),
            dma((2,)), dma((2,)), dma((2, 4)), dma((2, 4)),
            dma((2, 2, CHUNKS, n_fo, 2)), dma((2, 2, CHUNKS, n_fo, 2)),
            dma((2, CHUNKS)), dma((2, CHUNKS)),
        ],
        compiler_params=pltpu.CompilerParams(
            collective_id=0, has_side_effects=True, vmem_limit_bytes=64_000_000),
        name="layer",
    )(*tokens, *weights)


def on_device(n_fo, n_tp, x_late, x_early, cotangent, up_weight, down_weight, up_grad_sum, down_grad_sum):
    output, input_grad, up_grad, down_grad = layer(
        n_fo, n_tp, (x_early, cotangent, x_late), (up_weight, down_weight))
    return (output, input_grad, up_grad_sum + up_grad, down_grad_sum + down_grad)


def solution(mesh):
    n_fo, n_tp = mesh.shape["fs"] // 2, mesh.shape["tp"]
    assert n_tp == 4 and n_fo % 2 == 0
    rows, both = P(("fs", "tp"), None), P("fs", "tp")
    return jax.shard_map(
        functools.partial(on_device, n_fo, n_tp),
        mesh=mesh,
        in_specs=(rows, rows, rows, both, both, both, both),
        out_specs=(rows, rows, both, both),
        check_vma=False,
    )
```

```python
import functools

import jax
import jax.numpy as jnp
from jax import lax
from jax.experimental import pallas as pl
from jax.experimental.pallas import tpu as pltpu
from jax.sharding import PartitionSpec as P


MESH = pl.DeviceIdType.MESH
VMEM = pl.BlockSpec(memory_space=pltpu.VMEM)
EARLY, COT, LATE = 0, 1, 2
UP, DOWN = 0, 1
CHUNKS = 2
SKEW = 2


def dot(left, right, left_dim, right_dim):
    return lax.dot_general(
        left, right, (((left_dim,), (right_dim,)), ((), ())), preferred_element_type=jnp.float32
    )


def remote(src, dst, send, recv, fs, tp):
    return pltpu.make_async_remote_copy(
        src_ref=src, dst_ref=dst, send_sem=send, recv_sem=recv,
        device_id={"fs": fs, "tp": tp}, device_id_type=MESH,
    )


def layer_kernel(n_fo, n_tp, *refs):
    tokens, weights = refs[0:3], refs[3:5]
    summed, grads = refs[5:7], refs[7:9]
    (tok, wts, g_out, g_in, pre, hid, partial, landed, pair_sum, arrived, staged, other,
     local, t_send, t_recv, a_send, a_recv, zg_send, zg_recv,
     c_send, c_recv, p_send, p_recv, zr_send, zr_recv, x_send, x_recv) = refs[9:]
    fs, tp = lax.axis_index("fs"), lax.axis_index("tp")
    fo, fi = fs // 2, fs % 2
    y, core = tp // 2, tp % 2
    pair = fo * 2 + 1 - fi
    across_y = (1 - y) * 2 + core
    sibling = y * 2 + 1 - core
    rows, width = tokens[0].shape
    w_rows, cols = weights[0].shape
    half = cols // 2
    wide = half // CHUNKS
    count = 4 * rows * 2
    cut = rows // 96 * 16
    fold = rows // 96 * 32
    first, last = fo == 0, fo == n_fo - 1

    def side(part):
        return 1 - fi if part else fi

    def open_way(way):
        return jnp.logical_not(last) if way == 0 else jnp.logical_not(first)

    def ahead(way):
        return (fo + 1 - 2 * way) * 2 + fi

    spots = [(0, 0), (1, 0), (0, 1), (1, 1)]

    def slot(a, k, at_core):
        dx, dy = spots[k]
        return tok.at[a, (1 - fi if dx else fi), (1 - y if dy else y), at_core]

    def token(a, j):
        sems = t_send.at[a, j], t_recv.at[a, j]
        if j == 0:
            return remote(tokens[a], slot(a, 0, core), *sems, pair, tp)
        if j == 1:
            return remote(tokens[a], slot(a, 0, core), *sems, fs, across_y)
        if j == 2:
            part = slot(a, 2, core).at[pl.ds(0, cut)]
            return remote(part, part, *sems, pair, tp)
        if j == 3:
            part = slot(a, 1, core).at[pl.ds(cut, rows - cut)]
            return remote(part, part, *sems, fs, across_y)
        k = j - 4
        dst = slot(a, k, core)
        return remote(tokens[a] if k == 0 else dst, dst, *sems, fs, sibling)

    def token_in(a, j):
        sems = t_send.at[a, j], t_recv.at[a, j]
        if j < 2:
            dst = slot(a, 1 + j, core)
        elif j == 2:
            dst = slot(a, 3, core).at[pl.ds(0, cut)]
        elif j == 3:
            dst = slot(a, 3, core).at[pl.ds(cut, rows - cut)]
        else:
            dst = slot(a, j - 4, 1 - core)
        return remote(dst, dst, *sems, fs, sibling)

    def from_y(a):
        token_in(a, 1).wait_recv()
        token(a, 2).start()
        token(a, 6).start()

    def from_x(a):
        token_in(a, 0).wait_recv()
        token(a, 3).start()
        token(a, 5).start()

    def diagonal(a):
        token_in(a, 3).wait_recv()
        token_in(a, 2).wait_recv()
        token(a, 7).start()

    def from_sibling(a):
        for k in range(4):
            token_in(a, 4 + k).wait_recv()

    def columns(w, which, c):
        return weights[w].at[:, pl.ds(pl.multiple_of(which * half + c * wide, wide), wide)]

    def across(w, c):
        return remote(columns(w, 1 - fi, c), wts.at[w, c, fo, fi], a_send.at[w, c], a_recv.at[w, c], pair, tp)

    def across_in(w, c):
        dst = wts.at[w, c, fo, 1 - fi]
        return remote(dst, dst, a_send.at[w, c], a_recv.at[w, c], pair, tp)

    def along(w, c, source, part, way, src=None):
        dst = wts.at[w, c, source, side(part)]
        return remote(dst if src is None else src, dst, zg_send.at[way, w, c, source, part],
                      zg_recv.at[w, c, source, part], ahead(way), tp)

    def begin(w, c, distance=None):
        for way in range(2):
            behind = fo if way == 0 else n_fo - 1 - fo

            @pl.when(open_way(way) if distance is None else open_way(way) & (behind == distance))
            def _():
                along(w, c, fo, 0, way, columns(w, fi, c)).start()

    def crossed(w, c):
        across_in(w, c).wait_recv()
        for way in range(2):
            @pl.when(open_way(way))
            def _():
                along(w, c, fo, 1, way).start()

    def incoming(way, distance):
        source = fo - distance if way == 0 else fo + distance
        return source, (source >= 0) & (source < n_fo)

    def forward(w, c, part, distance):
        for way in range(2):
            source, inside = incoming(way, distance)

            @pl.when(inside & open_way(way))
            def _():
                along(w, c, source, part, way).wait_recv()
                along(w, c, source, part, way).start()

    def forward_far(w, c, part):
        for distance in range(2, n_fo - 1):
            forward(w, c, part, distance)

    def settle(w, c):
        for part in range(2):
            for distance in range(1, n_fo):
                for way in range(2):
                    source, inside = incoming(way, distance)

                    @pl.when(inside & jnp.logical_not(open_way(way)))
                    def _():
                        along(w, c, source, part, way).wait_recv()

    def flat(a):
        return tok[a].reshape(count, width)

    def weight(w, c):
        return wts[w, c].reshape(width, wide)

    def activate(c):
        relu = jnp.maximum(dot(flat(EARLY), weight(UP, c), 1, 0), 0.0)
        pre[...] = relu
        hid[0, c] = (relu * relu).astype(jnp.bfloat16)

    def hidden_grad(c):
        grad_act = dot(flat(COT), weight(DOWN, c), 1, 0)
        hid[1, c] = (grad_act * 2.0 * pre[...]).astype(jnp.bfloat16)

    def activate_late(c):
        relu = jnp.maximum(dot(flat(LATE), weight(UP, c), 1, 0), 0.0)
        hid[2, c] = (relu * relu).astype(jnp.bfloat16)

    n_half = n_fo // 2
    d_half = width // 2

    def weight_grad(w, c, step):
        at = jnp.where(fo < n_half, 1 - step, step)
        lanes = pl.ds(pl.multiple_of(at * d_half, d_half), d_half)
        left = tok[EARLY if w == UP else COT, :, :, :, :, lanes].reshape(count, d_half)
        value = dot(left, hid[1 if w == UP else 0, c], 0, 0)
        g_out[w, c, pl.ds(at * n_half, n_half)] = value.astype(jnp.bfloat16).reshape(n_half, 2, w_rows, wide)
        for k in range(n_half):
            for part in (1, 0):
                for way in range(2):
                    block = farthest(way, step * n_half + k)

                    @pl.when((first if way == 0 else last) & (fo != block))
                    def _():
                        grad(w, c, block, part, way, g_out.at[w, c, block, side(part)]).start()

    def token_partial(a, h, w):
        sources = max(1, 512 // (2 * w_rows))
        lanes = sources * 2 * w_rows
        for b in range(n_fo // sources):
            total = None
            for c in range(CHUNKS):
                right = wts[w, c, b * sources:(b + 1) * sources].reshape(lanes, wide)
                term = dot(hid[h, c], right, 1, 1)
                total = term if total is None else total + term
            partial[a, :, :, :, :, b * lanes:(b + 1) * lanes] = (
                total.astype(jnp.bfloat16).reshape(2, 2, 2, rows, lanes))
        near(a).start()

    def farthest(way, k):
        return n_fo - 1 - k if way == 0 else k

    def grad(w, c, block, part, way, src=None):
        held = g_in.at[way, w, c, block, part]
        return remote(held if src is None else src, held, zr_send.at[way, w, c, block, part],
                      zr_recv.at[way, w, c, block, part], ahead(way), tp)

    def carry(c, start, stop):
        def position(q, carried):
            for way in range(2):
                hop = fo if way == 0 else n_fo - 1 - fo
                item = q - SKEW * (hop - 1)
                w = 1 - item // (2 * n_fo)
                block = farthest(way, item % (2 * n_fo) // 2)
                part = 1 - item % 2
                inside = (hop > 0) & (hop < n_fo - 1) & (item >= 0) & (item < 4 * n_fo)
                beyond = fo < block if way == 0 else fo > block

                @pl.when(inside & beyond)
                def _():
                    row = jnp.where(part == 1, 1 - fi, fi)
                    grad(w, c, block, part, way).wait_recv()
                    g_in[way, w, c, block, part] = (
                        g_out[w, c, block, row].astype(jnp.float32)
                        + g_in[way, w, c, block, part].astype(jnp.float32)
                    ).astype(jnp.bfloat16)
                    grad(w, c, block, part, way).start()
            return carried

        lax.fori_loop(start, stop, position, 0)

    def swap(w, c):
        return remote(staged.at[w, c], other.at[w, c], x_send.at[w, c], x_recv.at[w, c], pair, tp)

    def owned(w, c, part):
        for way in range(2):
            @pl.when(first if way == 0 else last)
            def _():
                g_in[way, w, c, fo, part] = jnp.zeros(g_in.shape[5:], g_in.dtype)

            @pl.when(jnp.logical_not(first if way == 0 else last))
            def _():
                grad(w, c, fo, part, way).wait_recv()
        total = (g_out[w, c, fo, side(part)].astype(jnp.float32)
                 + g_in[0, w, c, fo, part].astype(jnp.float32)
                 + g_in[1, w, c, fo, part].astype(jnp.float32))
        if part:
            staged[w, c] = total.astype(jnp.bfloat16)
            swap(w, c).start()
        else:
            grads[w][:, pl.ds(pl.multiple_of(fi * half + c * wide, wide), wide)] = total

    def swapped(w, c):
        swap(w, c).wait_recv()
        grads[w][:, pl.ds(pl.multiple_of((1 - fi) * half + c * wide, wide), wide)] = (
            other[w, c].astype(jnp.float32))

    def spot(k):
        dx, dy = spots[k]
        return (1 - fi if dx else fi), (1 - y if dy else y)

    def near(a):
        return remote(partial.at[a, :, :, 1 - core], landed.at[a], c_send.at[a], c_recv.at[a], fs, sibling)

    near_rows, far_rows = pl.ds(0, fold), pl.ds(fold, rows - fold)

    def far(a, j):
        to_x = j in (0, 1, 5)
        lines = near_rows if j in (0, 1, 4) else far_rows
        if j < 4:
            src = pair_sum.at[a, *spot({0: 1, 1: 3, 2: 2, 3: 3}[j]), lines]
            dst = arrived.at[a, j % 2, lines]
        else:
            src = arrived.at[a, 1, lines]
            dst = arrived.at[a, 2, lines]
        return remote(src, dst, p_send.at[a, j], p_recv.at[a, j], pair if to_x else fs, tp if to_x else across_y)

    def joined(a, at_fi, at_y):
        return (partial[a, at_fi, at_y, core].astype(jnp.float32)
                + landed[a, at_fi, at_y].astype(jnp.float32))

    def spread(a):
        near(a).wait_recv()
        for k, sends in ((3, (1, 3)), (1, (0,)), (2, (2,))):
            pair_sum[(a, *spot(k))] = joined(a, *spot(k)).astype(jnp.bfloat16)
            for j in sends:
                far(a, j).start()

    def relay(a):
        for j, k, lines in ((1, 2, near_rows), (3, 1, far_rows)):
            far(a, j).wait_recv()
            arrived[a, 1, lines] = (
                pair_sum[(a, *spot(k), lines)].astype(jnp.float32)
                + arrived[a, 1, lines].astype(jnp.float32)
            ).astype(jnp.bfloat16)
            far(a, j // 2 + 4).start()

    def collect(a):
        for j in (0, 2, 4, 5):
            far(a, j).wait_recv()
        total = joined(a, fi, y) + arrived[a, 0].astype(jnp.float32) + arrived[a, 2].astype(jnp.float32)
        summed[a][...] = total.astype(jnp.bfloat16)

    barrier = pltpu.get_barrier_semaphore()

    def greet(to_fs, to_tp):
        pl.semaphore_signal(barrier, inc=1, device_id={"fs": to_fs, "tp": to_tp}, device_id_type=MESH)

    greet(pair, tp)
    greet(fs, across_y)
    greet(fs, sibling)
    for way in range(2):
        @pl.when(open_way(way))
        def _():
            greet(ahead(way), tp)
    pl.semaphore_wait(barrier, 3 + (fo > 0).astype(jnp.int32) + (fo < n_fo - 1).astype(jnp.int32))

    begin(UP, 0)
    across(UP, 0).start()
    for a in (EARLY, COT):
        token(a, 0).start()
        token(a, 1).start()
        if a == EARLY:
            across(DOWN, 0).start()
    for a in (EARLY, COT, LATE):
        token(a, 4).start()
    own = [pltpu.make_async_copy(tokens[a], slot(a, 0, core), local.at[a]) for a in range(3)]
    own += [pltpu.make_async_copy(columns(w, fi, c), wts.at[w, c, fo, fi], local.at[3 + w * CHUNKS + c])
            for w in range(2) for c in range(CHUNKS)]
    for copy in own:
        copy.start()

    inner = range(2, n_fo - 1)
    crossed(UP, 0)
    begin(DOWN, 0, 0)
    forward(UP, 0, 0, 1)
    from_y(EARLY)
    for w in (UP, DOWN):
        across(w, 1).start()
    forward_far(UP, 0, 0)
    forward(UP, 0, 1, 1)
    begin(DOWN, 0, 1)
    from_x(EARLY)
    for distance in inner:
        forward(UP, 0, 1, distance)
        begin(DOWN, 0, distance)
    crossed(DOWN, 0)
    for w in (UP, DOWN):
        begin(w, 1, 0)
    forward(DOWN, 0, 0, 1)
    from_y(COT)
    forward_far(DOWN, 0, 0)
    forward(DOWN, 0, 1, 1)
    begin(UP, 1, 1)
    from_x(COT)
    token(LATE, 0).start()
    token(LATE, 1).start()
    for distance in inner:
        forward(DOWN, 0, 1, distance)
        begin(UP, 1, distance)
    diagonal(EARLY)
    for copy in own:
        copy.wait()
    from_sibling(EARLY)
    settle(UP, 0)
    crossed(UP, 1)
    forward(UP, 1, 0, 1)
    activate(0)
    crossed(DOWN, 1)
    forward_far(UP, 1, 0)
    diagonal(COT)
    forward(UP, 1, 1, 1)
    begin(DOWN, 1, 1)
    from_sibling(COT)
    weight_grad(DOWN, 0, 0)
    weight_grad(DOWN, 0, 1)
    settle(DOWN, 0)
    hidden_grad(0)
    for distance in inner:
        forward(UP, 1, 1, distance)
        begin(DOWN, 1, distance)
    weight_grad(UP, 0, 0)
    weight_grad(UP, 0, 1)
    forward(DOWN, 1, 0, 1)
    from_y(LATE)
    from_x(LATE)
    forward_far(DOWN, 1, 0)
    carry(0, 0, 1)
    forward(DOWN, 1, 1, 1)
    carry(0, 1, 2)
    forward_far(DOWN, 1, 1)
    carry(0, 2, n_fo)
    diagonal(LATE)
    carry(0, n_fo, n_fo + 1)
    from_sibling(LATE)
    activate_late(0)
    carry(0, n_fo + 1, 2 * n_fo)
    settle(UP, 1)
    activate(1)
    weight_grad(DOWN, 1, 0)
    weight_grad(DOWN, 1, 1)
    carry(0, 2 * n_fo, 2 * n_fo + 2)
    activate_late(1)
    carry(0, 2 * n_fo + 2, 4 * n_fo + SKEW * (n_fo - 3))
    settle(DOWN, 1)
    hidden_grad(1)
    token_partial(1, 1, UP)
    weight_grad(UP, 1, 0)
    spread(1)
    token_partial(0, 2, DOWN)
    weight_grad(UP, 1, 1)
    spread(0)
    owned(DOWN, 0, 1)
    owned(DOWN, 0, 0)
    carry(1, 0, 1)
    relay(1)
    carry(1, 1, 2)
    owned(UP, 0, 1)
    owned(UP, 0, 0)
    carry(1, 2, n_fo)
    relay(0)
    carry(1, n_fo, 2 * n_fo)
    for w in (DOWN, UP):
        swapped(w, 0)
    carry(1, 2 * n_fo, 2 * n_fo + SKEW)
    owned(DOWN, 1, 1)
    owned(DOWN, 1, 0)
    carry(1, 2 * n_fo + SKEW, 4 * n_fo + SKEW * (n_fo - 3))
    collect(1)
    collect(0)
    owned(UP, 1, 1)
    owned(UP, 1, 0)
    for w in (DOWN, UP):
        swapped(w, 1)

    for a in range(3):
        for j in range(8):
            token(a, j).wait_send()
    for w in range(2):
        for c in range(CHUNKS):
            across(w, c).wait_send()
            swap(w, c).wait_send()
            for way in range(2):
                @pl.when(open_way(way))
                def _():
                    for part in range(2):
                        along(w, c, fo, part, way).wait_send()

                for distance in range(1, n_fo):
                    source, inside = incoming(way, distance)

                    @pl.when(inside & open_way(way))
                    def _():
                        for part in range(2):
                            along(w, c, source, part, way).wait_send()

                for block in range(n_fo):
                    @pl.when(fo < block if way == 0 else fo > block)
                    def _():
                        for part in range(2):
                            grad(w, c, block, part, way).wait_send()
    for a in range(2):
        near(a).wait_send()
        for j in range(6):
            far(a, j).wait_send()


def layer(n_fo, n_tp, tokens, weights):
    rows, width = tokens[0].shape
    w_rows, cols = weights[0].shape
    wide = cols // 2 // CHUNKS
    count = 8 * rows
    dma = pltpu.SemaphoreType.DMA
    bf16, f32 = jnp.bfloat16, jnp.float32
    return pl.pallas_call(
        functools.partial(layer_kernel, n_fo, n_tp),
        out_shape=[jax.ShapeDtypeStruct((rows, width), bf16)] * 2
        + [jax.ShapeDtypeStruct((w_rows, cols), f32)] * 2,
        in_specs=[VMEM] * 5,
        out_specs=[VMEM] * 4,
        scratch_shapes=[
            pltpu.VMEM((3, 2, 2, 2, rows, width), bf16),
            pltpu.VMEM((2, CHUNKS, n_fo, 2, w_rows, wide), bf16),
            pltpu.VMEM((2, CHUNKS, n_fo, 2, w_rows, wide), bf16),
            pltpu.VMEM((2, 2, CHUNKS, n_fo, 2, w_rows, wide), bf16),
            pltpu.VMEM((count, wide), f32),
            pltpu.VMEM((3, CHUNKS, count, wide), bf16),
            pltpu.VMEM((2, 2, 2, 2, rows, width), bf16),
            pltpu.VMEM((2, 2, 2, rows, width), bf16),
            pltpu.VMEM((2, 2, 2, rows, width), bf16),
            pltpu.VMEM((2, 3, rows, width), bf16),
            pltpu.VMEM((2, CHUNKS, w_rows, wide), bf16),
            pltpu.VMEM((2, CHUNKS, w_rows, wide), bf16),
            dma((3 + 2 * CHUNKS,)), dma((3, 8)), dma((3, 8)), dma((2, CHUNKS)), dma((2, CHUNKS)),
            dma((2, 2, CHUNKS, n_fo, 2)), dma((2, CHUNKS, n_fo, 2)),
            dma((2,)), dma((2,)), dma((2, 6)), dma((2, 6)),
            dma((2, 2, CHUNKS, n_fo, 2)), dma((2, 2, CHUNKS, n_fo, 2)),
            dma((2, CHUNKS)), dma((2, CHUNKS)),
        ],
        compiler_params=pltpu.CompilerParams(
            collective_id=0, has_side_effects=True, vmem_limit_bytes=52_000_000),
        name="layer",
    )(*tokens, *weights)


def on_device(n_fo, n_tp, x_late, x_early, cotangent, up_weight, down_weight, up_grad_sum, down_grad_sum):
    output, input_grad, up_grad, down_grad = layer(
        n_fo, n_tp, (x_early, cotangent, x_late), (up_weight, down_weight))
    return (output, input_grad, up_grad_sum + up_grad, down_grad_sum + down_grad)


def solution(mesh):
    n_fo, n_tp = mesh.shape["fs"] // 2, mesh.shape["tp"]
    assert n_tp == 4 and n_fo % 2 == 0
    rows, both = P(("fs", "tp"), None), P("fs", "tp")
    return jax.shard_map(
        functools.partial(on_device, n_fo, n_tp),
        mesh=mesh,
        in_specs=(rows, rows, rows, both, both, both, both),
        out_specs=(rows, rows, both, both),
        check_vma=False,
    )
```

```python
import functools

import jax
import jax.numpy as jnp
from jax import lax
from jax.experimental import pallas as pl
from jax.experimental.pallas import tpu as pltpu
from jax.sharding import PartitionSpec as P


MESH = pl.DeviceIdType.MESH
VMEM = pl.BlockSpec(memory_space=pltpu.VMEM)
HBM = pl.BlockSpec(memory_space=pltpu.HBM)
EARLY, COT, LATE = 0, 1, 2
UP, DOWN = 0, 1
CHUNKS = 2
SKEW = 2


def dot(left, right, left_dim, right_dim):
    return lax.dot_general(
        left, right, (((left_dim,), (right_dim,)), ((), ())), preferred_element_type=jnp.float32
    )


def remote(src, dst, send, recv, fs, tp):
    return pltpu.make_async_remote_copy(
        src_ref=src, dst_ref=dst, send_sem=send, recv_sem=recv,
        device_id={"fs": fs, "tp": tp}, device_id_type=MESH,
    )


def layer_kernel(n_fo, n_tp, *refs):
    tokens, weights = refs[0:3], refs[3:5]
    summed, grads = refs[5:7], refs[7:9]
    (tok, wts, lent, g_out, g_in, pre, hid, partial, landed, pair_sum, arrived, staged, other,
     local, t_send, t_recv, a_send, a_recv, zg_send, zg_recv,
     c_send, c_recv, p_send, p_recv, zr_send, zr_recv, x_send, x_recv) = refs[9:]
    fs, tp = lax.axis_index("fs"), lax.axis_index("tp")
    fo, fi = fs // 2, fs % 2
    y, core = tp // 2, tp % 2
    pair = fo * 2 + 1 - fi
    across_y = (1 - y) * 2 + core
    sibling = y * 2 + 1 - core
    rows, width = tokens[0].shape
    w_rows, cols = weights[0].shape
    half = cols // 2
    wide = half // CHUNKS
    count = 4 * rows * 2
    cut = rows // 96 * 16
    fold = rows // 96 * 16
    first, last = fo == 0, fo == n_fo - 1

    def side(part):
        return 1 - fi if part else fi

    def open_way(way):
        return jnp.logical_not(last) if way == 0 else jnp.logical_not(first)

    def ahead(way):
        return (fo + 1 - 2 * way) * 2 + fi

    spots = [(0, 0), (1, 0), (0, 1), (1, 1)]

    def slot(a, k, at_core):
        dx, dy = spots[k]
        return tok.at[a, (1 - fi if dx else fi), (1 - y if dy else y), at_core]

    def token(a, j):
        sems = t_send.at[a, j], t_recv.at[a, j]
        if j == 0:
            return remote(slot(a, 0, core), slot(a, 0, core), *sems, pair, tp)
        if j == 1:
            return remote(slot(a, 0, core), slot(a, 0, core), *sems, fs, across_y)
        if j == 2:
            part = slot(a, 2, core).at[pl.ds(0, cut)]
            return remote(part, part, *sems, pair, tp)
        if j == 3:
            part = slot(a, 1, core).at[pl.ds(cut, rows - cut)]
            return remote(part, part, *sems, fs, across_y)
        k = j - 4
        dst = slot(a, k, core)
        return remote(dst, dst, *sems, fs, sibling)

    def token_in(a, j):
        sems = t_send.at[a, j], t_recv.at[a, j]
        if j < 2:
            dst = slot(a, 1 + j, core)
        elif j == 2:
            dst = slot(a, 3, core).at[pl.ds(0, cut)]
        elif j == 3:
            dst = slot(a, 3, core).at[pl.ds(cut, rows - cut)]
        else:
            dst = slot(a, j - 4, 1 - core)
        return remote(dst, dst, *sems, fs, sibling)

    def from_y(a):
        token_in(a, 1).wait_recv()
        token(a, 2).start()
        token(a, 6).start()

    def from_x(a):
        token_in(a, 0).wait_recv()
        token(a, 3).start()
        token(a, 5).start()

    def diagonal(a):
        token_in(a, 3).wait_recv()
        token_in(a, 2).wait_recv()
        token(a, 7).start()

    def from_sibling(a):
        for k in range(4):
            token_in(a, 4 + k).wait_recv()

    def columns(w, which, c):
        return weights[w].at[:, pl.ds(pl.multiple_of(which * half + c * wide, wide), wide)]

    def load_tokens(a):
        return pltpu.make_async_copy(tokens[a], slot(a, 0, core), local.at[a])

    def load_weight(w, c, mine):
        dst = wts.at[w, c, fo, fi] if mine else lent.at[w, c]
        sem = local.at[3 + (w * CHUNKS + c) * 2 + mine]
        return pltpu.make_async_copy(columns(w, fi if mine else 1 - fi, c), dst, sem)

    def across(w, c):
        return remote(lent.at[w, c], wts.at[w, c, fo, fi], a_send.at[w, c], a_recv.at[w, c], pair, tp)

    def across_in(w, c):
        dst = wts.at[w, c, fo, 1 - fi]
        return remote(dst, dst, a_send.at[w, c], a_recv.at[w, c], pair, tp)

    def along(w, c, source, part, way):
        dst = wts.at[w, c, source, side(part)]
        return remote(dst, dst, zg_send.at[way, w, c, source, part],
                      zg_recv.at[w, c, source, part], ahead(way), tp)

    def begin(w, c, distance=None):
        for way in range(2):
            behind = fo if way == 0 else n_fo - 1 - fo

            @pl.when(open_way(way) if distance is None else open_way(way) & (behind == distance))
            def _():
                along(w, c, fo, 0, way).start()

    def crossed(w, c):
        across_in(w, c).wait_recv()
        for way in range(2):
            @pl.when(open_way(way))
            def _():
                along(w, c, fo, 1, way).start()

    def incoming(way, distance):
        source = fo - distance if way == 0 else fo + distance
        return source, (source >= 0) & (source < n_fo)

    def forward(w, c, part, distance):
        for way in range(2):
            source, inside = incoming(way, distance)

            @pl.when(inside & open_way(way))
            def _():
                along(w, c, source, part, way).wait_recv()
                along(w, c, source, part, way).start()

    def forward_far(w, c, part):
        for distance in range(2, n_fo - 1):
            forward(w, c, part, distance)

    def settle(w, c):
        for part in range(2):
            for distance in range(1, n_fo):
                for way in range(2):
                    source, inside = incoming(way, distance)

                    @pl.when(inside & jnp.logical_not(open_way(way)))
                    def _():
                        along(w, c, source, part, way).wait_recv()

    def flat(a):
        return tok[a].reshape(count, width)

    def weight(w, c):
        return wts[w, c].reshape(width, wide)

    def activate(c):
        relu = jnp.maximum(dot(flat(EARLY), weight(UP, c), 1, 0), 0.0)
        pre[...] = relu
        hid[0, c] = (relu * relu).astype(jnp.bfloat16)

    def hidden_grad(c):
        grad_act = dot(flat(COT), weight(DOWN, c), 1, 0)
        hid[1, c] = (grad_act * 2.0 * pre[...]).astype(jnp.bfloat16)

    def activate_late(c):
        relu = jnp.maximum(dot(flat(LATE), weight(UP, c), 1, 0), 0.0)
        hid[2, c] = (relu * relu).astype(jnp.bfloat16)

    n_half = n_fo // 2
    d_half = width // 2

    def weight_grad(w, c, step):
        at = jnp.where(fo < n_half, 1 - step, step)
        lanes = pl.ds(pl.multiple_of(at * d_half, d_half), d_half)
        left = tok[EARLY if w == UP else COT, :, :, :, :, lanes].reshape(count, d_half)
        value = dot(left, hid[1 if w == UP else 0, c], 0, 0)
        g_out[w, c, pl.ds(at * n_half, n_half)] = value.astype(jnp.bfloat16).reshape(n_half, 2, w_rows, wide)
        for k in range(n_half):
            for part in (1, 0):
                for way in range(2):
                    block = farthest(way, step * n_half + k)

                    @pl.when((first if way == 0 else last) & (fo != block))
                    def _():
                        grad(w, c, block, part, way, g_out.at[w, c, block, side(part)]).start()

    def token_begin(a, h, w):
        value = dot(hid[h, 0], weight(w, 0), 1, 1)
        partial[a] = value.astype(jnp.bfloat16).reshape(2, 2, 2, rows, width)

    def token_partial(a, h, w):
        for dx, spots_of in ((1, (3, 1)), (0, (2, 0))):
            at_fi = 1 - fi if dx else fi
            lines = pl.ds(pl.multiple_of(at_fi * 4 * rows, 4 * rows), 4 * rows)
            total = partial[a, at_fi].astype(jnp.float32).reshape(4 * rows, width)
            for c in range(1, CHUNKS):
                total += dot(hid[h, c, lines], weight(w, c), 1, 1)
            partial[a, at_fi] = total.astype(jnp.bfloat16).reshape(2, 2, rows, width)
            for k in spots_of:
                near(a, k).start()

    def farthest(way, k):
        return n_fo - 1 - k if way == 0 else k

    def grad(w, c, block, part, way, src=None):
        held = g_in.at[way, w, c, block, part]
        return remote(held if src is None else src, held, zr_send.at[way, w, c, block, part],
                      zr_recv.at[way, w, c, block, part], ahead(way), tp)

    def carry(c, start, stop):
        def position(q, carried):
            for way in range(2):
                hop = fo if way == 0 else n_fo - 1 - fo
                item = q - SKEW * (hop - 1)
                w = 1 - item // (2 * n_fo)
                block = farthest(way, item % (2 * n_fo) // 2)
                part = 1 - item % 2
                inside = (hop > 0) & (hop < n_fo - 1) & (item >= 0) & (item < 4 * n_fo)
                beyond = fo < block if way == 0 else fo > block

                @pl.when(inside & beyond)
                def _():
                    row = jnp.where(part == 1, 1 - fi, fi)
                    grad(w, c, block, part, way).wait_recv()
                    g_in[way, w, c, block, part] = (
                        g_out[w, c, block, row].astype(jnp.float32)
                        + g_in[way, w, c, block, part].astype(jnp.float32)
                    ).astype(jnp.bfloat16)
                    grad(w, c, block, part, way).start()
            return carried

        lax.fori_loop(start, stop, position, 0)

    def swap(w, c):
        return remote(staged.at[w, c], other.at[w, c], x_send.at[w, c], x_recv.at[w, c], pair, tp)

    def owned(w, c, part):
        for way in range(2):
            @pl.when(first if way == 0 else last)
            def _():
                g_in[way, w, c, fo, part] = jnp.zeros(g_in.shape[5:], g_in.dtype)

            @pl.when(jnp.logical_not(first if way == 0 else last))
            def _():
                grad(w, c, fo, part, way).wait_recv()
        total = (g_out[w, c, fo, side(part)].astype(jnp.float32)
                 + g_in[0, w, c, fo, part].astype(jnp.float32)
                 + g_in[1, w, c, fo, part].astype(jnp.float32))
        if part:
            staged[w, c] = total.astype(jnp.bfloat16)
            swap(w, c).start()
        else:
            grads[w][:, pl.ds(pl.multiple_of(fi * half + c * wide, wide), wide)] = total

    def swapped(w, c):
        swap(w, c).wait_recv()
        grads[w][:, pl.ds(pl.multiple_of((1 - fi) * half + c * wide, wide), wide)] = (
            other[w, c].astype(jnp.float32))

    def spot(k):
        dx, dy = spots[k]
        return (1 - fi if dx else fi), (1 - y if dy else y)

    def near(a, k):
        return remote(partial.at[(a, *spot(k), 1 - core)], landed.at[(a, *spot(k))], c_send.at[a, k],
                      c_recv.at[a, k], fs, sibling)

    near_rows, far_rows = pl.ds(0, fold), pl.ds(fold, rows - fold)

    def far(a, j):
        to_x = j in (0, 1, 5)
        lines = near_rows if j in (0, 1, 4) else far_rows
        if j < 4:
            src = pair_sum.at[a, *spot({0: 1, 1: 3, 2: 2, 3: 3}[j]), lines]
            dst = arrived.at[a, j % 2, lines]
        else:
            src = arrived.at[a, 1, lines]
            dst = arrived.at[a, 2, lines]
        return remote(src, dst, p_send.at[a, j], p_recv.at[a, j], pair if to_x else fs, tp if to_x else across_y)

    def joined(a, at_fi, at_y):
        return (partial[a, at_fi, at_y, core].astype(jnp.float32)
                + landed[a, at_fi, at_y].astype(jnp.float32))

    def spread(a, diagonal_spot):
        for k, sends in ((3, (1, 3)),) if diagonal_spot else ((1, (0,)), (2, (2,))):
            near(a, k).wait_recv()
            pair_sum[(a, *spot(k))] = joined(a, *spot(k)).astype(jnp.bfloat16)
            for j in sends:
                far(a, j).start()

    def relay(a):
        for j, k, lines in ((1, 2, near_rows), (3, 1, far_rows)):
            far(a, j).wait_recv()
            arrived[a, 1, lines] = (
                pair_sum[(a, *spot(k), lines)].astype(jnp.float32)
                + arrived[a, 1, lines].astype(jnp.float32)
            ).astype(jnp.bfloat16)
            far(a, j // 2 + 4).start()

    def collect(a):
        near(a, 0).wait_recv()
        for j in (0, 2, 4, 5):
            far(a, j).wait_recv()
        total = joined(a, fi, y) + arrived[a, 0].astype(jnp.float32) + arrived[a, 2].astype(jnp.float32)
        summed[a][...] = total.astype(jnp.bfloat16)

    barrier = pltpu.get_barrier_semaphore()

    def greet(to_fs, to_tp):
        pl.semaphore_signal(barrier, inc=1, device_id={"fs": to_fs, "tp": to_tp}, device_id_type=MESH)

    greet(pair, tp)
    greet(fs, across_y)
    greet(fs, sibling)
    for way in range(2):
        @pl.when(open_way(way))
        def _():
            greet(ahead(way), tp)
    for c in range(CHUNKS):
        for w in (UP, DOWN):
            for mine in (True, False):
                load_weight(w, c, mine).start()
        load_tokens(EARLY + c).start()
    load_tokens(LATE).start()
    pl.semaphore_wait(barrier, 3 + (fo > 0).astype(jnp.int32) + (fo < n_fo - 1).astype(jnp.int32))

    for w in (UP, DOWN):
        load_weight(w, 0, True).wait()
        load_weight(w, 0, False).wait()
        begin(w, 0)
        across(w, 0).start()
        load_tokens(EARLY + w).wait()
        token(EARLY + w, 1).start()
        token(EARLY + w, 0).start()
    load_tokens(LATE).wait()
    for a in (EARLY, COT, LATE):
        token(a, 4).start()
    for w in (UP, DOWN):
        for mine in (True, False):
            load_weight(w, 1, mine).wait()

    inner = range(2, n_fo - 1)
    crossed(UP, 0)
    forward(UP, 0, 0, 1)
    from_y(EARLY)
    for w in (UP, DOWN):
        across(w, 1).start()
    forward_far(UP, 0, 0)
    forward(UP, 0, 1, 1)
    from_x(EARLY)
    for distance in inner:
        forward(UP, 0, 1, distance)
    forward(DOWN, 0, 0, 1)
    crossed(DOWN, 0)
    for w in (UP, DOWN):
        begin(w, 1, 0)
    from_y(COT)
    forward_far(DOWN, 0, 0)
    forward(DOWN, 0, 1, 1)
    begin(UP, 1, 1)
    from_x(COT)
    token(LATE, 0).start()
    token(LATE, 1).start()
    for distance in inner:
        forward(DOWN, 0, 1, distance)
        begin(UP, 1, distance)
    diagonal(EARLY)
    from_sibling(EARLY)
    settle(UP, 0)
    forward(UP, 1, 0, 1)
    crossed(UP, 1)
    activate(0)
    crossed(DOWN, 1)
    forward(UP, 1, 1, 1)
    begin(DOWN, 1, 1)
    diagonal(COT)
    from_sibling(COT)
    weight_grad(DOWN, 0, 0)
    weight_grad(DOWN, 0, 1)
    forward(DOWN, 1, 0, 1)
    forward_far(UP, 1, 0)
    settle(DOWN, 0)
    hidden_grad(0)
    for distance in inner:
        forward(UP, 1, 1, distance)
        begin(DOWN, 1, distance)
    from_y(LATE)
    from_x(LATE)
    weight_grad(UP, 0, 0)
    weight_grad(UP, 0, 1)
    forward(DOWN, 1, 1, 1)
    carry(0, 0, 2)
    forward_far(DOWN, 1, 0)
    carry(0, 2, 3)
    forward_far(DOWN, 1, 1)
    diagonal(LATE)
    carry(0, 3, n_fo)
    from_sibling(LATE)
    activate_late(0)
    token_begin(0, 2, DOWN)
    carry(0, n_fo, 2 * n_fo + 2)
    token_begin(1, 1, UP)
    settle(UP, 1)
    activate(1)
    carry(0, 2 * n_fo + 2, 2 * n_fo + 3)
    weight_grad(DOWN, 1, 0)
    weight_grad(DOWN, 1, 1)
    carry(0, 2 * n_fo + 3, 4 * n_fo + SKEW * (n_fo - 3))
    activate_late(1)
    settle(DOWN, 1)
    token_partial(0, 2, DOWN)
    spread(0, True)
    hidden_grad(1)
    carry(1, 0, 1)
    token_partial(1, 1, UP)
    spread(1, True)
    carry(1, 1, 2)
    spread(0, False)
    owned(DOWN, 0, 1)
    weight_grad(UP, 1, 0)
    carry(1, 2, 3)
    spread(1, False)
    weight_grad(UP, 1, 1)
    owned(UP, 0, 1)
    carry(1, 3, n_fo)
    relay(0)
    carry(1, n_fo, 2 * n_fo)
    for w in (DOWN, UP):
        owned(w, 0, 0)
    relay(1)
    carry(1, 2 * n_fo, 2 * n_fo + 1)
    owned(DOWN, 1, 1)
    owned(DOWN, 1, 0)
    carry(1, 2 * n_fo + 1, 4 * n_fo + SKEW * (n_fo - 3))
    for w in (DOWN, UP):
        swapped(w, 0)
    owned(UP, 1, 1)
    collect(0)
    owned(UP, 1, 0)
    swapped(DOWN, 1)
    collect(1)
    swapped(UP, 1)

    for a in range(3):
        for j in range(8):
            token(a, j).wait_send()
    for w in range(2):
        for c in range(CHUNKS):
            across(w, c).wait_send()
            swap(w, c).wait_send()
            for way in range(2):
                @pl.when(open_way(way))
                def _():
                    for part in range(2):
                        along(w, c, fo, part, way).wait_send()

                for distance in range(1, n_fo):
                    source, inside = incoming(way, distance)

                    @pl.when(inside & open_way(way))
                    def _():
                        for part in range(2):
                            along(w, c, source, part, way).wait_send()

                for block in range(n_fo):
                    @pl.when(fo < block if way == 0 else fo > block)
                    def _():
                        for part in range(2):
                            grad(w, c, block, part, way).wait_send()
    for a in range(2):
        for k in range(4):
            near(a, k).wait_send()
        for j in range(6):
            far(a, j).wait_send()


def layer(n_fo, n_tp, tokens, weights):
    rows, width = tokens[0].shape
    w_rows, cols = weights[0].shape
    wide = cols // 2 // CHUNKS
    count = 8 * rows
    dma = pltpu.SemaphoreType.DMA
    bf16, f32 = jnp.bfloat16, jnp.float32
    return pl.pallas_call(
        functools.partial(layer_kernel, n_fo, n_tp),
        out_shape=[jax.ShapeDtypeStruct((rows, width), bf16)] * 2
        + [jax.ShapeDtypeStruct((w_rows, cols), f32)] * 2,
        in_specs=[HBM] * 5,
        out_specs=[VMEM] * 4,
        scratch_shapes=[
            pltpu.VMEM((3, 2, 2, 2, rows, width), bf16),
            pltpu.VMEM((2, CHUNKS, n_fo, 2, w_rows, wide), bf16),
            pltpu.VMEM((2, CHUNKS, w_rows, wide), bf16),
            pltpu.VMEM((2, CHUNKS, n_fo, 2, w_rows, wide), bf16),
            pltpu.VMEM((2, 2, CHUNKS, n_fo, 2, w_rows, wide), bf16),
            pltpu.VMEM((count, wide), f32),
            pltpu.VMEM((3, CHUNKS, count, wide), bf16),
            pltpu.VMEM((2, 2, 2, 2, rows, width), bf16),
            pltpu.VMEM((2, 2, 2, rows, width), bf16),
            pltpu.VMEM((2, 2, 2, rows, width), bf16),
            pltpu.VMEM((2, 3, rows, width), bf16),
            pltpu.VMEM((2, CHUNKS, w_rows, wide), bf16),
            pltpu.VMEM((2, CHUNKS, w_rows, wide), bf16),
            dma((3 + 4 * CHUNKS,)), dma((3, 8)), dma((3, 8)), dma((2, CHUNKS)), dma((2, CHUNKS)),
            dma((2, 2, CHUNKS, n_fo, 2)), dma((2, CHUNKS, n_fo, 2)),
            dma((2, 4)), dma((2, 4)), dma((2, 6)), dma((2, 6)),
            dma((2, 2, CHUNKS, n_fo, 2)), dma((2, 2, CHUNKS, n_fo, 2)),
            dma((2, CHUNKS)), dma((2, CHUNKS)),
        ],
        compiler_params=pltpu.CompilerParams(
            collective_id=0, has_side_effects=True, vmem_limit_bytes=50_000_000),
        name="layer",
    )(*(pltpu.with_memory_space_constraint(a, pltpu.HBM) for a in (*tokens, *weights)))


def on_device(n_fo, n_tp, x_late, x_early, cotangent, up_weight, down_weight, up_grad_sum, down_grad_sum):
    output, input_grad, up_grad, down_grad = layer(
        n_fo, n_tp, (x_early, cotangent, x_late), (up_weight, down_weight))
    return (output, input_grad, up_grad_sum + up_grad, down_grad_sum + down_grad)


def solution(mesh):
    n_fo, n_tp = mesh.shape["fs"] // 2, mesh.shape["tp"]
    assert n_tp == 4 and n_fo % 2 == 0
    rows, both = P(("fs", "tp"), None), P("fs", "tp")
    return jax.shard_map(
        functools.partial(on_device, n_fo, n_tp),
        mesh=mesh,
        in_specs=(rows, rows, rows, both, both, both, both),
        out_specs=(rows, rows, both, both),
        check_vma=False,
    )
```

```python
import functools

import jax
import jax.numpy as jnp
from jax import lax
from jax.experimental import pallas as pl
from jax.experimental.pallas import tpu as pltpu
from jax.sharding import PartitionSpec as P


MESH = pl.DeviceIdType.MESH
VMEM = pl.BlockSpec(memory_space=pltpu.VMEM)
HBM = pl.BlockSpec(memory_space=pltpu.HBM)
EARLY, COT, LATE = 0, 1, 2
UP, DOWN = 0, 1
CHUNKS = 2
SKEW = 2


def dot(left, right, left_dim, right_dim):
    return lax.dot_general(
        left, right, (((left_dim,), (right_dim,)), ((), ())), preferred_element_type=jnp.float32
    )


def remote(src, dst, send, recv, fs, tp):
    return pltpu.make_async_remote_copy(
        src_ref=src, dst_ref=dst, send_sem=send, recv_sem=recv,
        device_id={"fs": fs, "tp": tp}, device_id_type=MESH,
    )


def layer_kernel(n_fo, n_tp, *refs):
    tokens, weights = refs[0:3], refs[3:5]
    summed, grads = refs[5:7], refs[7:9]
    (tok, wts, lent, g_out, g_in, pre, hid, partial, landed, pair_sum, arrived, staged, other,
     local, t_send, t_recv, a_send, a_recv, zg_send, zg_recv,
     c_send, c_recv, p_send, p_recv, zr_send, zr_recv, x_send, x_recv) = refs[9:]
    fs, tp = lax.axis_index("fs"), lax.axis_index("tp")
    fo, fi = fs // 2, fs % 2
    y, core = tp // 2, tp % 2
    pair = fo * 2 + 1 - fi
    across_y = (1 - y) * 2 + core
    sibling = y * 2 + 1 - core
    rows, width = tokens[0].shape
    w_rows, cols = weights[0].shape
    half = cols // 2
    wide = half // CHUNKS
    count = 4 * rows * 2
    cut = rows // 96 * 16
    fold = rows // 96 * 16
    first, last = fo == 0, fo == n_fo - 1

    def side(part):
        return 1 - fi if part else fi

    def open_way(way):
        return jnp.logical_not(last) if way == 0 else jnp.logical_not(first)

    def ahead(way):
        return (fo + 1 - 2 * way) * 2 + fi

    spots = [(0, 0), (1, 0), (0, 1), (1, 1)]

    def slot(a, k, at_core):
        dx, dy = spots[k]
        return tok.at[a, (1 - fi if dx else fi), (1 - y if dy else y), at_core]

    def token(a, j):
        sems = t_send.at[a % 2, j], t_recv.at[a, j]
        if j == 0:
            return remote(slot(a, 0, core), slot(a, 0, core), *sems, pair, tp)
        if j == 1:
            return remote(slot(a, 0, core), slot(a, 0, core), *sems, fs, across_y)
        if j == 2:
            part = slot(a, 2, core).at[pl.ds(0, cut)]
            return remote(part, part, *sems, pair, tp)
        if j == 3:
            part = slot(a, 1, core).at[pl.ds(cut, rows - cut)]
            return remote(part, part, *sems, fs, across_y)
        k = j - 4
        dst = slot(a, k, core)
        return remote(dst, dst, *sems, fs, sibling)

    def token_in(a, j):
        sems = t_send.at[a % 2, j], t_recv.at[a, j]
        if j < 2:
            dst = slot(a, 1 + j, core)
        elif j == 2:
            dst = slot(a, 3, core).at[pl.ds(0, cut)]
        elif j == 3:
            dst = slot(a, 3, core).at[pl.ds(cut, rows - cut)]
        else:
            dst = slot(a, j - 4, 1 - core)
        return remote(dst, dst, *sems, fs, sibling)

    def send_token(a, j):
        if a == LATE:
            token(EARLY, j).wait_send()
        token(a, j).start()

    def from_y(a):
        token_in(a, 1).wait_recv()
        send_token(a, 2)
        send_token(a, 6)

    def from_x(a):
        token_in(a, 0).wait_recv()
        send_token(a, 3)
        send_token(a, 5)

    def diagonal(a):
        token_in(a, 3).wait_recv()
        token_in(a, 2).wait_recv()
        send_token(a, 7)

    def from_sibling(a):
        for k in range(4):
            token_in(a, 4 + k).wait_recv()

    def columns(w, which, c):
        return weights[w].at[:, pl.ds(pl.multiple_of(which * half + c * wide, wide), wide)]

    def load_tokens(a):
        return pltpu.make_async_copy(tokens[a], slot(a, 0, core), local.at[a])

    def load_weight(w, c, mine):
        dst = wts.at[w, c, fo, fi] if mine else lent.at[w, c]
        sem = local.at[3 + (w * CHUNKS + c) * 2 + mine]
        return pltpu.make_async_copy(columns(w, fi if mine else 1 - fi, c), dst, sem)

    def across(w, c):
        return remote(lent.at[w, c], wts.at[w, c, fo, fi], a_send.at[w, c], a_recv.at[w, c], pair, tp)

    def across_in(w, c):
        dst = wts.at[w, c, fo, 1 - fi]
        return remote(dst, dst, a_send.at[w, c], a_recv.at[w, c], pair, tp)

    def along(w, c, source, part, way):
        dst = wts.at[w, c, source, side(part)]
        sem = jnp.where(source == fo, n_fo, source) if way else source
        return remote(dst, dst, zg_send.at[w, sem, part], zg_recv.at[w, c, source, part], ahead(way), tp)

    def send_along(w, c, source, part, way):
        if c:
            along(w, c - 1, source, part, way).wait_send()
        along(w, c, source, part, way).start()

    def begin(w, c, distance=None):
        for way in range(2):
            behind = fo if way == 0 else n_fo - 1 - fo

            @pl.when(open_way(way) if distance is None else open_way(way) & (behind == distance))
            def _():
                send_along(w, c, fo, 0, way)

    def crossed(w, c):
        across_in(w, c).wait_recv()
        for way in range(2):
            @pl.when(open_way(way))
            def _():
                send_along(w, c, fo, 1, way)

    def incoming(way, distance):
        source = fo - distance if way == 0 else fo + distance
        return source, (source >= 0) & (source < n_fo)

    def forward(w, c, part, distance):
        for way in range(2):
            source, inside = incoming(way, distance)

            @pl.when(inside & open_way(way))
            def _():
                along(w, c, source, part, way).wait_recv()
                send_along(w, c, source, part, way)

    def forward_far(w, c, part):
        for distance in range(2, n_fo - 1):
            forward(w, c, part, distance)

    def settle(w, c):
        for part in range(2):
            for distance in range(1, n_fo):
                for way in range(2):
                    source, inside = incoming(way, distance)

                    @pl.when(inside & jnp.logical_not(open_way(way)))
                    def _():
                        along(w, c, source, part, way).wait_recv()

    def flat(a):
        return tok[a].reshape(count, width)

    def weight(w, c):
        return wts[w, c].reshape(width, wide)

    def activate(c):
        relu = jnp.maximum(dot(flat(EARLY), weight(UP, c), 1, 0), 0.0)
        pre[...] = relu
        hid[0, c] = (relu * relu).astype(jnp.bfloat16)

    def hidden_grad(c):
        grad_act = dot(flat(COT), weight(DOWN, c), 1, 0)
        hid[1, c] = (grad_act * 2.0 * pre[...]).astype(jnp.bfloat16)

    def activate_late(c):
        relu = jnp.maximum(dot(flat(LATE), weight(UP, c), 1, 0), 0.0)
        hid[2, c] = (relu * relu).astype(jnp.bfloat16)

    n_half = n_fo // 2
    d_half = width // 2

    def weight_grad(w, c, step):
        at = jnp.where(fo < n_half, 1 - step, step)
        lanes = pl.ds(pl.multiple_of(at * d_half, d_half), d_half)
        left = tok[EARLY if w == UP else COT, :, :, :, :, lanes].reshape(count, d_half)
        value = dot(left, hid[1 if w == UP else 0, c], 0, 0)
        g_out[w, c, pl.ds(at * n_half, n_half)] = value.astype(jnp.bfloat16).reshape(n_half, 2, w_rows, wide)
        for k in range(n_half):
            for part in (1, 0):
                for way in range(2):
                    block = farthest(way, step * n_half + k)

                    @pl.when((first if way == 0 else last) & (fo != block))
                    def _():
                        send_grad(w, c, block, part, way, g_out.at[w, c, block, side(part)])

    def token_begin(a, h, w):
        value = dot(hid[h, 0], weight(w, 0), 1, 1)
        partial[a] = value.astype(jnp.bfloat16).reshape(2, 2, 2, rows, width)

    def token_partial(a, h, w):
        for dx, spots_of in ((1, (3, 1)), (0, (2, 0))):
            at_fi = 1 - fi if dx else fi
            lines = pl.ds(pl.multiple_of(at_fi * 4 * rows, 4 * rows), 4 * rows)
            total = partial[a, at_fi].astype(jnp.float32).reshape(4 * rows, width)
            for c in range(1, CHUNKS):
                total += dot(hid[h, c, lines], weight(w, c), 1, 1)
            partial[a, at_fi] = total.astype(jnp.bfloat16).reshape(2, 2, rows, width)
            for k in spots_of:
                near(a, k).start()

    def farthest(way, k):
        return n_fo - 1 - k if way == 0 else k

    def grad(w, c, block, part, way, src=None, taker=None):
        held = g_in.at[way, w, c, block, part]
        taker = fo - 1 if taker is None else taker
        sem = jnp.where(block == taker, n_fo, block) if way else block
        return remote(held if src is None else src, held, zr_send.at[w, block, part],
                      zr_recv.at[w, c, sem, part], ahead(way), tp)

    def send_grad(w, c, block, part, way, src=None):
        if c:
            grad(w, c - 1, block, part, way, src).wait_send()
        grad(w, c, block, part, way, src).start()

    def carry(c, start, stop):
        def position(q, carried):
            for way in range(2):
                hop = fo if way == 0 else n_fo - 1 - fo
                item = q - SKEW * (hop - 1)
                w = 1 - item // (2 * n_fo)
                block = farthest(way, item % (2 * n_fo) // 2)
                part = 1 - item % 2
                inside = (hop > 0) & (hop < n_fo - 1) & (item >= 0) & (item < 4 * n_fo)
                beyond = fo < block if way == 0 else fo > block

                @pl.when(inside & beyond)
                def _():
                    row = jnp.where(part == 1, 1 - fi, fi)
                    grad(w, c, block, part, way, taker=fo).wait_recv()
                    g_in[way, w, c, block, part] = (
                        g_out[w, c, block, row].astype(jnp.float32)
                        + g_in[way, w, c, block, part].astype(jnp.float32)
                    ).astype(jnp.bfloat16)
                    send_grad(w, c, block, part, way)
            return carried

        lax.fori_loop(start, stop, position, 0)

    def swap(w, c):
        return remote(staged.at[w, c], other.at[w, c], x_send.at[w, c], x_recv.at[w, c], pair, tp)

    def owned(w, c, part):
        for way in range(2):
            @pl.when(first if way == 0 else last)
            def _():
                g_in[way, w, c, fo, part] = jnp.zeros(g_in.shape[5:], g_in.dtype)

            @pl.when(jnp.logical_not(first if way == 0 else last))
            def _():
                grad(w, c, fo, part, way, taker=fo).wait_recv()
        total = (g_out[w, c, fo, side(part)].astype(jnp.float32)
                 + g_in[0, w, c, fo, part].astype(jnp.float32)
                 + g_in[1, w, c, fo, part].astype(jnp.float32))
        if part:
            staged[w, c] = total.astype(jnp.bfloat16)
            swap(w, c).start()
        else:
            grads[w][:, pl.ds(pl.multiple_of(fi * half + c * wide, wide), wide)] = total

    def swapped(w, c):
        swap(w, c).wait_recv()
        grads[w][:, pl.ds(pl.multiple_of((1 - fi) * half + c * wide, wide), wide)] = (
            other[w, c].astype(jnp.float32))

    def spot(k):
        dx, dy = spots[k]
        return (1 - fi if dx else fi), (1 - y if dy else y)

    def near(a, k):
        return remote(partial.at[(a, *spot(k), 1 - core)], landed.at[(a, *spot(k))], c_send.at[a, k],
                      c_recv.at[a, k], fs, sibling)

    near_rows, far_rows = pl.ds(0, fold), pl.ds(fold, rows - fold)

    def far(a, j):
        to_x = j in (0, 1, 5)
        lines = near_rows if j in (0, 1, 4) else far_rows
        if j < 4:
            src = pair_sum.at[a, *spot({0: 1, 1: 3, 2: 2, 3: 3}[j]), lines]
            dst = arrived.at[a, j % 2, lines]
        else:
            src = arrived.at[a, 1, lines]
            dst = arrived.at[a, 2, lines]
        return remote(src, dst, p_send.at[a, j], p_recv.at[a, j], pair if to_x else fs, tp if to_x else across_y)

    def joined(a, at_fi, at_y):
        return (partial[a, at_fi, at_y, core].astype(jnp.float32)
                + landed[a, at_fi, at_y].astype(jnp.float32))

    def spread(a, k):
        near(a, k).wait_recv()
        pair_sum[(a, *spot(k))] = joined(a, *spot(k)).astype(jnp.bfloat16)
        for j in {3: (1, 3), 1: (0,), 2: (2,)}[k]:
            far(a, j).start()

    def relay(a):
        for j, k, lines in ((1, 2, near_rows), (3, 1, far_rows)):
            far(a, j).wait_recv()
            arrived[a, 1, lines] = (
                pair_sum[(a, *spot(k), lines)].astype(jnp.float32)
                + arrived[a, 1, lines].astype(jnp.float32)
            ).astype(jnp.bfloat16)
            far(a, j // 2 + 4).start()

    def collect(a):
        near(a, 0).wait_recv()
        for j in (0, 2, 4, 5):
            far(a, j).wait_recv()
        total = joined(a, fi, y) + arrived[a, 0].astype(jnp.float32) + arrived[a, 2].astype(jnp.float32)
        summed[a][...] = total.astype(jnp.bfloat16)

    barrier = pltpu.get_barrier_semaphore()

    def greet(to_fs, to_tp):
        pl.semaphore_signal(barrier, inc=1, device_id={"fs": to_fs, "tp": to_tp}, device_id_type=MESH)

    greet(pair, tp)
    greet(fs, across_y)
    greet(fs, sibling)
    for way in range(2):
        @pl.when(open_way(way))
        def _():
            greet(ahead(way), tp)
    for c in range(CHUNKS):
        for w in (UP, DOWN):
            for mine in (True, False):
                load_weight(w, c, mine).start()
        load_tokens(EARLY + c).start()
    load_tokens(LATE).start()
    pl.semaphore_wait(barrier, 3 + (fo > 0).astype(jnp.int32) + (fo < n_fo - 1).astype(jnp.int32))

    for w in (UP, DOWN):
        load_weight(w, 0, True).wait()
        load_weight(w, 0, False).wait()
        begin(w, 0)
        across(w, 0).start()
        load_tokens(EARLY + w).wait()
        token(EARLY + w, 1).start()
        token(EARLY + w, 0).start()
    load_tokens(LATE).wait()
    for a in (EARLY, COT):
        token(a, 4).start()
    for w in (UP, DOWN):
        for mine in (True, False):
            load_weight(w, 1, mine).wait()

    inner = range(2, n_fo - 1)
    forward(UP, 0, 0, 1)
    crossed(UP, 0)
    forward_far(UP, 0, 0)
    forward(UP, 0, 1, 1)
    from_y(EARLY)
    for w in (UP, DOWN):
        across(w, 1).start()
    from_x(EARLY)
    for distance in inner:
        forward(UP, 0, 1, distance)
    forward(DOWN, 0, 0, 1)
    crossed(DOWN, 0)
    for w in (UP, DOWN):
        begin(w, 1, 0)
    from_y(COT)
    forward_far(DOWN, 0, 0)
    forward(DOWN, 0, 1, 1)
    begin(UP, 1, 1)
    from_x(COT)
    for j in (0, 1, 4):
        send_token(LATE, j)
    for distance in inner:
        forward(DOWN, 0, 1, distance)
        begin(UP, 1, distance)
    diagonal(EARLY)
    from_sibling(EARLY)
    settle(UP, 0)
    forward(UP, 1, 0, 1)
    crossed(UP, 1)
    activate(0)
    crossed(DOWN, 1)
    forward(UP, 1, 1, 1)
    begin(DOWN, 1, 1)
    diagonal(COT)
    from_sibling(COT)
    weight_grad(DOWN, 0, 0)
    weight_grad(DOWN, 0, 1)
    forward(DOWN, 1, 0, 1)
    forward_far(UP, 1, 0)
    settle(DOWN, 0)
    hidden_grad(0)
    for distance in inner:
        forward(UP, 1, 1, distance)
        begin(DOWN, 1, distance)
    from_y(LATE)
    from_x(LATE)
    weight_grad(UP, 0, 0)
    weight_grad(UP, 0, 1)
    forward(DOWN, 1, 1, 1)
    carry(0, 0, 2)
    forward_far(DOWN, 1, 0)
    carry(0, 2, 3)
    forward_far(DOWN, 1, 1)
    diagonal(LATE)
    carry(0, 3, n_fo)
    from_sibling(LATE)
    activate_late(0)
    token_begin(0, 2, DOWN)
    carry(0, n_fo, 2 * n_fo + 2)
    token_begin(1, 1, UP)
    settle(UP, 1)
    activate(1)
    carry(0, 2 * n_fo + 2, 2 * n_fo + 3)
    weight_grad(DOWN, 1, 0)
    weight_grad(DOWN, 1, 1)
    carry(0, 2 * n_fo + 3, 4 * n_fo + SKEW * (n_fo - 3))
    activate_late(1)
    settle(DOWN, 1)
    token_partial(0, 2, DOWN)
    spread(0, 3)
    hidden_grad(1)
    spread(0, 1)
    carry(1, 0, 1)
    owned(DOWN, 0, 1)
    token_partial(1, 1, UP)
    spread(1, 3)
    carry(1, 1, 2)
    spread(1, 1)
    spread(0, 2)
    weight_grad(UP, 1, 0)
    carry(1, 2, 3)
    spread(1, 2)
    weight_grad(UP, 1, 1)
    owned(UP, 0, 1)
    carry(1, 3, n_fo)
    relay(0)
    carry(1, n_fo, 2 * n_fo)
    for w in (DOWN, UP):
        owned(w, 0, 0)
    relay(1)
    carry(1, 2 * n_fo, 2 * n_fo + 1)
    owned(DOWN, 1, 1)
    owned(DOWN, 1, 0)
    carry(1, 2 * n_fo + 1, 4 * n_fo + SKEW * (n_fo - 3))
    for w in (DOWN, UP):
        swapped(w, 0)
    owned(UP, 1, 1)
    collect(0)
    owned(UP, 1, 0)
    swapped(DOWN, 1)
    collect(1)
    swapped(UP, 1)

    for a in (COT, LATE):
        for j in range(8):
            token(a, j).wait_send()
    for w in range(2):
        for c in range(CHUNKS):
            across(w, c).wait_send()
            swap(w, c).wait_send()
        c = CHUNKS - 1
        for way in range(2):
            @pl.when(open_way(way))
            def _():
                for part in range(2):
                    along(w, c, fo, part, way).wait_send()

            for distance in range(1, n_fo):
                source, inside = incoming(way, distance)

                @pl.when(inside & open_way(way))
                def _():
                    for part in range(2):
                        along(w, c, source, part, way).wait_send()

            for block in range(n_fo):
                @pl.when(fo < block if way == 0 else fo > block)
                def _():
                    for part in range(2):
                        grad(w, c, block, part, way).wait_send()
    for a in range(2):
        for k in range(4):
            near(a, k).wait_send()
        for j in range(6):
            far(a, j).wait_send()


def layer(n_fo, n_tp, tokens, weights):
    rows, width = tokens[0].shape
    w_rows, cols = weights[0].shape
    wide = cols // 2 // CHUNKS
    count = 8 * rows
    dma = pltpu.SemaphoreType.DMA
    bf16, f32 = jnp.bfloat16, jnp.float32
    return pl.pallas_call(
        functools.partial(layer_kernel, n_fo, n_tp),
        out_shape=[jax.ShapeDtypeStruct((rows, width), bf16)] * 2
        + [jax.ShapeDtypeStruct((w_rows, cols), f32)] * 2,
        in_specs=[HBM] * 5,
        out_specs=[VMEM] * 4,
        scratch_shapes=[
            pltpu.VMEM((3, 2, 2, 2, rows, width), bf16),
            pltpu.VMEM((2, CHUNKS, n_fo, 2, w_rows, wide), bf16),
            pltpu.VMEM((2, CHUNKS, w_rows, wide), bf16),
            pltpu.VMEM((2, CHUNKS, n_fo, 2, w_rows, wide), bf16),
            pltpu.VMEM((2, 2, CHUNKS, n_fo, 2, w_rows, wide), bf16),
            pltpu.VMEM((count, wide), f32),
            pltpu.VMEM((3, CHUNKS, count, wide), bf16),
            pltpu.VMEM((2, 2, 2, 2, rows, width), bf16),
            pltpu.VMEM((2, 2, 2, rows, width), bf16),
            pltpu.VMEM((2, 2, 2, rows, width), bf16),
            pltpu.VMEM((2, 3, rows, width), bf16),
            pltpu.VMEM((2, CHUNKS, w_rows, wide), bf16),
            pltpu.VMEM((2, CHUNKS, w_rows, wide), bf16),
            dma((3 + 4 * CHUNKS,)), dma((2, 8)), dma((3, 8)), dma((2, CHUNKS)), dma((2, CHUNKS)),
            dma((2, n_fo + 1, 2)), dma((2, CHUNKS, n_fo, 2)),
            dma((2, 4)), dma((2, 4)), dma((2, 6)), dma((2, 6)),
            dma((2, n_fo, 2)), dma((2, CHUNKS, n_fo + 1, 2)),
            dma((2, CHUNKS)), dma((2, CHUNKS)),
        ],
        compiler_params=pltpu.CompilerParams(
            collective_id=0, has_side_effects=True, vmem_limit_bytes=50_000_000),
        name="layer",
    )(*(pltpu.with_memory_space_constraint(a, pltpu.HBM) for a in (*tokens, *weights)))


def finish_kernel(*refs):
    found, sums, results, (total, sems) = refs[0:4], refs[4:6], refs[6:10], refs[10:]
    copies = [pltpu.make_async_copy(found[a], results[a], sems.at[a]) for a in range(2)]
    for copy in copies:
        copy.start()
    for w in range(2):
        total[w] = sums[w][...] + found[2 + w][...]
        copies.append(pltpu.make_async_copy(total.at[w], results[2 + w], sems.at[2 + w]))
        copies[-1].start()
    for copy in copies:
        copy.wait()


def finish(found, sums):
    return pl.pallas_call(
        finish_kernel,
        out_shape=[jax.ShapeDtypeStruct(a.shape, a.dtype) for a in found],
        in_specs=[VMEM] * 6,
        out_specs=[pl.BlockSpec(memory_space=pl.ANY)] * 4,
        scratch_shapes=[pltpu.VMEM((2, *sums[0].shape), jnp.float32), pltpu.SemaphoreType.DMA((4,))],
        compiler_params=pltpu.CompilerParams(vmem_limit_bytes=8_000_000),
        name="finish",
    )(*found, *sums)


def on_device(n_fo, n_tp, x_late, x_early, cotangent, up_weight, down_weight, up_grad_sum, down_grad_sum):
    found = layer(n_fo, n_tp, (x_early, cotangent, x_late), (up_weight, down_weight))
    return tuple(finish(found, (up_grad_sum, down_grad_sum)))


def solution(mesh):
    n_fo, n_tp = mesh.shape["fs"] // 2, mesh.shape["tp"]
    assert n_tp == 4 and n_fo % 2 == 0
    rows, both = P(("fs", "tp"), None), P("fs", "tp")
    return jax.shard_map(
        functools.partial(on_device, n_fo, n_tp),
        mesh=mesh,
        in_specs=(rows, rows, rows, both, both, both, both),
        out_specs=(rows, rows, both, both),
        check_vma=False,
    )
```

```python
import functools

import jax
import jax.numpy as jnp
from jax import lax
from jax.experimental import pallas as pl
from jax.experimental.pallas import tpu as pltpu
from jax.sharding import PartitionSpec as P


MESH = pl.DeviceIdType.MESH
VMEM = pl.BlockSpec(memory_space=pltpu.VMEM)
HBM = pl.BlockSpec(memory_space=pltpu.HBM)
EARLY, COT, LATE = 0, 1, 2
UP, DOWN = 0, 1
CHUNKS = 2
SKEW = 2


def dot(left, right, left_dim, right_dim):
    return lax.dot_general(
        left, right, (((left_dim,), (right_dim,)), ((), ())), preferred_element_type=jnp.float32
    )


def remote(src, dst, send, recv, fs, tp):
    return pltpu.make_async_remote_copy(
        src_ref=src, dst_ref=dst, send_sem=send, recv_sem=recv,
        device_id={"fs": fs, "tp": tp}, device_id_type=MESH,
    )


def layer_kernel(n_fo, n_tp, *refs):
    tokens, weights = refs[0:3], refs[3:5]
    summed, grads = refs[5:7], refs[7:9]
    (tok, wts, lent, g_out, g_in, pre, hid, partial, landed, pair_sum, arrived, staged, other,
     local, t_send, t_recv, a_send, a_recv, zg_send, zg_recv,
     c_send, c_recv, p_send, p_recv, zr_send, zr_recv, x_send, x_recv) = refs[9:]
    fs, tp = lax.axis_index("fs"), lax.axis_index("tp")
    fo, fi = fs // 2, fs % 2
    y, core = tp // 2, tp % 2
    pair = fo * 2 + 1 - fi
    across_y = (1 - y) * 2 + core
    sibling = y * 2 + 1 - core
    rows, width = tokens[0].shape
    w_rows, cols = weights[0].shape
    half = cols // 2
    wide = half // CHUNKS
    count = 4 * rows * 2
    cut = rows // 96 * 16
    fold = rows // 96 * 16
    first, last = fo == 0, fo == n_fo - 1

    def side(part):
        return 1 - fi if part else fi

    n_half = n_fo // 2
    nearer = (fo >= n_half).astype(jnp.int32)
    ends = first | last

    def open_way(way):
        return ((way == 0) & (fo < n_fo - 1)) | ((way == 1) & (fo > 0))

    def ahead(way):
        return (fo + 1 - 2 * way) * 2 + fi

    spots = [(0, 0), (1, 0), (0, 1), (1, 1)]

    def slot(a, k, at_core):
        dx, dy = spots[k]
        return tok.at[a, (1 - fi if dx else fi), (1 - y if dy else y), at_core]

    def token(a, j):
        sems = t_send.at[a % 2, j], t_recv.at[a, j]
        if j == 0:
            return remote(slot(a, 0, core), slot(a, 0, core), *sems, pair, tp)
        if j == 1:
            return remote(slot(a, 0, core), slot(a, 0, core), *sems, fs, across_y)
        if j == 2:
            part = slot(a, 2, core).at[pl.ds(0, cut)]
            return remote(part, part, *sems, pair, tp)
        if j == 3:
            part = slot(a, 1, core).at[pl.ds(cut, rows - cut)]
            return remote(part, part, *sems, fs, across_y)
        k = j - 4
        dst = slot(a, k, core)
        return remote(dst, dst, *sems, fs, sibling)

    def token_in(a, j):
        sems = t_send.at[a % 2, j], t_recv.at[a, j]
        if j < 2:
            dst = slot(a, 1 + j, core)
        elif j == 2:
            dst = slot(a, 3, core).at[pl.ds(0, cut)]
        elif j == 3:
            dst = slot(a, 3, core).at[pl.ds(cut, rows - cut)]
        else:
            dst = slot(a, j - 4, 1 - core)
        return remote(dst, dst, *sems, fs, sibling)

    def send_token(a, j):
        if a == LATE:
            token(EARLY, j).wait_send()
        token(a, j).start()

    def from_y(a):
        token_in(a, 1).wait_recv()
        send_token(a, 2)
        send_token(a, 6)

    def from_x(a):
        token_in(a, 0).wait_recv()
        send_token(a, 3)
        send_token(a, 5)

    def diagonal(a):
        token_in(a, 3).wait_recv()
        token_in(a, 2).wait_recv()
        send_token(a, 7)

    def from_sibling(a):
        for k in range(4):
            token_in(a, 4 + k).wait_recv()

    def columns(w, which, c):
        return weights[w].at[:, pl.ds(pl.multiple_of(which * half + c * wide, wide), wide)]

    def load_tokens(a):
        return pltpu.make_async_copy(tokens[a], slot(a, 0, core), local.at[a])

    def load_weight(w, c, mine):
        dst = wts.at[w, c, fo, fi] if mine else lent.at[w, c]
        sem = local.at[3 + (w * CHUNKS + c) * 2 + mine]
        return pltpu.make_async_copy(columns(w, fi if mine else 1 - fi, c), dst, sem)

    def across(w, c):
        return remote(lent.at[w, c], wts.at[w, c, fo, fi], a_send.at[w, c], a_recv.at[w, c], pair, tp)

    def across_in(w, c):
        dst = wts.at[w, c, fo, 1 - fi]
        return remote(dst, dst, a_send.at[w, c], a_recv.at[w, c], pair, tp)

    def along(w, c, source, part, way):
        dst = wts.at[w, c, source, side(part)]
        sem = jnp.where((source == fo) & (way == 1), n_fo, source)
        return remote(dst, dst, zg_send.at[w, sem, part], zg_recv.at[w, c, source, part], ahead(way), tp)

    def send_along(w, c, source, part, way):
        if c:
            along(w, c - 1, source, part, way).wait_send()
        along(w, c, source, part, way).start()

    def begin(w, c, distance=None):
        for way in range(2):
            behind = fo if way == 0 else n_fo - 1 - fo

            @pl.when(open_way(way) if distance is None else open_way(way) & (behind == distance))
            def _():
                send_along(w, c, fo, 0, way)

    def crossed(w, c):
        across_in(w, c).wait_recv()
        for way in range(2):
            @pl.when(open_way(way))
            def _():
                send_along(w, c, fo, 1, way)

    def incoming(way, distance):
        source = fo - distance + 2 * distance * way
        return source, (source >= 0) & (source < n_fo)

    def forward(w, c, part, distance):
        for way in (nearer, 1 - nearer):
            source, inside = incoming(way, distance)

            @pl.when(inside & open_way(way))
            def _():
                along(w, c, source, part, way).wait_recv()
                send_along(w, c, source, part, way)

    def forward_far(w, c, part):
        for distance in range(2, n_fo - 1):
            forward(w, c, part, distance)

    def settle(w, c):
        for part in range(2):
            for distance in range(1, n_fo):
                for way in range(2):
                    source, inside = incoming(way, distance)

                    @pl.when(inside & jnp.logical_not(open_way(way)))
                    def _():
                        along(w, c, source, part, way).wait_recv()

    def flat(a):
        return tok[a].reshape(count, width)

    def weight(w, c):
        return wts[w, c].reshape(width, wide)

    def activate(c):
        relu = jnp.maximum(dot(flat(EARLY), weight(UP, c), 1, 0), 0.0)
        pre[...] = relu
        hid[0, c] = (relu * relu).astype(jnp.bfloat16)

    def hidden_grad(c):
        grad_act = dot(flat(COT), weight(DOWN, c), 1, 0)
        hid[1, c] = (grad_act * 2.0 * pre[...]).astype(jnp.bfloat16)

    def activate_late(c):
        relu = jnp.maximum(dot(flat(LATE), weight(UP, c), 1, 0), 0.0)
        hid[2, c] = (relu * relu).astype(jnp.bfloat16)

    d_half = width // 2

    def weight_grad(w, c, step):
        at = jnp.where(fo < n_half, 1 - step, step)
        lanes = pl.ds(pl.multiple_of(at * d_half, d_half), d_half)
        left = tok[EARLY if w == UP else COT, :, :, :, :, lanes].reshape(count, d_half)
        value = dot(left, hid[1 if w == UP else 0, c], 0, 0)
        g_out[w, c, pl.ds(at * n_half, n_half)] = value.astype(jnp.bfloat16).reshape(n_half, 2, w_rows, wide)
        for k in range(n_half):
            for part in (1, 0):
                for way in range(2):
                    block = farthest(way, step * n_half + k)

                    @pl.when((first if way == 0 else last) & (fo != block))
                    def _():
                        send_grad(w, c, block, part, way, g_out.at[w, c, block, side(part)])

    def token_begin(a, h, w):
        value = dot(hid[h, 0], weight(w, 0), 1, 1)
        partial[a] = value.astype(jnp.bfloat16).reshape(2, 2, 2, rows, width)

    def token_partial(a, h, w):
        for dx, spots_of in ((1, (3, 1)), (0, (2, 0))):
            at_fi = 1 - fi if dx else fi
            lines = pl.ds(pl.multiple_of(at_fi * 4 * rows, 4 * rows), 4 * rows)
            total = partial[a, at_fi].astype(jnp.float32).reshape(4 * rows, width)
            for c in range(1, CHUNKS):
                total += dot(hid[h, c, lines], weight(w, c), 1, 1)
            partial[a, at_fi] = total.astype(jnp.bfloat16).reshape(2, 2, rows, width)
            for k in spots_of:
                near(a, k).start()

    def farthest(way, k):
        return n_fo - 1 - k if way == 0 else k

    def grad(w, c, block, part, way, src=None, taker=None):
        held = g_in.at[way, w, c, block, part]
        taker = fo - 1 if taker is None else taker
        sem = jnp.where((block == taker) & (way == 1), n_fo, block)
        return remote(held if src is None else src, held, zr_send.at[w, block, part],
                      zr_recv.at[w, c, sem, part], ahead(way), tp)

    def send_grad(w, c, block, part, way, src=None):
        if c:
            grad(w, c - 1, block, part, way, src).wait_send()
        grad(w, c, block, part, way, src).start()

    def carry(c, start, stop):
        def position(q, carried):
            for way in (nearer, 1 - nearer):
                hop = jnp.where(way == 0, fo, n_fo - 1 - fo)
                item = q - SKEW * (hop - 1)
                w = 1 - item // (2 * n_fo)
                k = item % (2 * n_fo) // 2
                block = jnp.where(way == 0, n_fo - 1 - k, k)
                part = 1 - item % 2
                inside = (hop > 0) & (hop < n_fo - 1) & (item >= 0) & (item < 4 * n_fo)
                beyond = jnp.where(way == 0, block - fo, fo - block) > 0

                @pl.when(inside & beyond)
                def _():
                    row = jnp.where(part == 1, 1 - fi, fi)
                    grad(w, c, block, part, way, taker=fo).wait_recv()
                    g_in[way, w, c, block, part] = (
                        g_out[w, c, block, row].astype(jnp.float32)
                        + g_in[way, w, c, block, part].astype(jnp.float32)
                    ).astype(jnp.bfloat16)
                    send_grad(w, c, block, part, way)
            return carried

        lax.fori_loop(start, stop, position, 0)

    def swap(w, c):
        return remote(staged.at[w, c], other.at[w, c], x_send.at[w, c], x_recv.at[w, c], pair, tp)

    def owned(w, c, part):
        for way in range(2):
            @pl.when(first if way == 0 else last)
            def _():
                g_in[way, w, c, fo, part] = jnp.zeros(g_in.shape[5:], g_in.dtype)

            @pl.when(jnp.logical_not(first if way == 0 else last))
            def _():
                grad(w, c, fo, part, way, taker=fo).wait_recv()
        total = (g_out[w, c, fo, side(part)].astype(jnp.float32)
                 + g_in[0, w, c, fo, part].astype(jnp.float32)
                 + g_in[1, w, c, fo, part].astype(jnp.float32))
        if part:
            staged[w, c] = total.astype(jnp.bfloat16)
            swap(w, c).start()
        else:
            grads[w][:, pl.ds(pl.multiple_of(fi * half + c * wide, wide), wide)] = total

    def swapped(w, c):
        swap(w, c).wait_recv()
        grads[w][:, pl.ds(pl.multiple_of((1 - fi) * half + c * wide, wide), wide)] = (
            other[w, c].astype(jnp.float32))

    def spot(k):
        dx, dy = spots[k]
        return (1 - fi if dx else fi), (1 - y if dy else y)

    def near(a, k):
        return remote(partial.at[(a, *spot(k), 1 - core)], landed.at[(a, *spot(k))], c_send.at[a, k],
                      c_recv.at[a, k], fs, sibling)

    near_rows, far_rows = pl.ds(0, fold), pl.ds(fold, rows - fold)

    def far(a, j):
        to_x = j in (0, 1, 5)
        lines = near_rows if j in (0, 1, 4) else far_rows
        if j < 4:
            src = pair_sum.at[a, *spot({0: 1, 1: 3, 2: 2, 3: 3}[j]), lines]
            dst = arrived.at[a, j % 2, lines]
        else:
            src = arrived.at[a, 1, lines]
            dst = arrived.at[a, 2, lines]
        return remote(src, dst, p_send.at[a, j], p_recv.at[a, j], pair if to_x else fs, tp if to_x else across_y)

    def joined(a, at_fi, at_y):
        return (partial[a, at_fi, at_y, core].astype(jnp.float32)
                + landed[a, at_fi, at_y].astype(jnp.float32))

    def spread(a, k):
        near(a, k).wait_recv()
        pair_sum[(a, *spot(k))] = joined(a, *spot(k)).astype(jnp.bfloat16)
        for j in {3: (1, 3), 1: (0,), 2: (2,)}[k]:
            far(a, j).start()

    def relay(a):
        for j, k, lines in ((1, 2, near_rows), (3, 1, far_rows)):
            far(a, j).wait_recv()
            arrived[a, 1, lines] = (
                pair_sum[(a, *spot(k), lines)].astype(jnp.float32)
                + arrived[a, 1, lines].astype(jnp.float32)
            ).astype(jnp.bfloat16)
            far(a, j // 2 + 4).start()

    def collect(a):
        near(a, 0).wait_recv()
        for j in (0, 2, 4, 5):
            far(a, j).wait_recv()
        total = joined(a, fi, y) + arrived[a, 0].astype(jnp.float32) + arrived[a, 2].astype(jnp.float32)
        summed[a][...] = total.astype(jnp.bfloat16)

    barrier = pltpu.get_barrier_semaphore()

    def greet(to_fs, to_tp):
        pl.semaphore_signal(barrier, inc=1, device_id={"fs": to_fs, "tp": to_tp}, device_id_type=MESH)

    greet(pair, tp)
    greet(fs, across_y)
    greet(fs, sibling)
    for way in range(2):
        @pl.when(open_way(way))
        def _():
            greet(ahead(way), tp)
    for c in range(CHUNKS):
        for w in (UP, DOWN):
            for mine in (True, False):
                load_weight(w, c, mine).start()
        load_tokens(EARLY + c).start()
    load_tokens(LATE).start()
    pl.semaphore_wait(barrier, 3 + (fo > 0).astype(jnp.int32) + (fo < n_fo - 1).astype(jnp.int32))

    for w in (UP, DOWN):
        load_weight(w, 0, True).wait()
        load_weight(w, 0, False).wait()
        begin(w, 0)
        across(w, 0).start()
        load_tokens(EARLY + w).wait()
        token(EARLY + w, 1).start()
        token(EARLY + w, 0).start()
    load_tokens(LATE).wait()
    for a in (EARLY, COT):
        token(a, 4).start()
    for w in (UP, DOWN):
        for mine in (True, False):
            load_weight(w, 1, mine).wait()

    inner = range(2, n_fo - 1)
    forward(UP, 0, 0, 1)
    crossed(UP, 0)
    forward_far(UP, 0, 0)
    forward(UP, 0, 1, 1)
    from_y(EARLY)
    for w in (UP, DOWN):
        across(w, 1).start()
    from_x(EARLY)
    for distance in inner:
        forward(UP, 0, 1, distance)
    forward(DOWN, 0, 0, 1)
    crossed(DOWN, 0)
    for w in (UP, DOWN):
        begin(w, 1, 0)
    from_y(COT)
    forward_far(DOWN, 0, 0)
    forward(DOWN, 0, 1, 1)
    begin(UP, 1, 1)
    from_x(COT)
    for j in (0, 1, 4):
        send_token(LATE, j)
    for distance in inner:
        forward(DOWN, 0, 1, distance)
        begin(UP, 1, distance)
    diagonal(EARLY)
    from_sibling(EARLY)
    settle(UP, 0)
    forward(UP, 1, 0, 1)
    crossed(UP, 1)
    activate(0)
    crossed(DOWN, 1)
    forward(UP, 1, 1, 1)
    begin(DOWN, 1, 1)
    diagonal(COT)
    from_sibling(COT)
    weight_grad(DOWN, 0, 0)
    weight_grad(DOWN, 0, 1)
    forward(DOWN, 1, 0, 1)
    forward_far(UP, 1, 0)
    settle(DOWN, 0)
    hidden_grad(0)
    for distance in inner:
        forward(UP, 1, 1, distance)
        begin(DOWN, 1, distance)
    from_y(LATE)
    from_x(LATE)
    weight_grad(UP, 0, 0)
    weight_grad(UP, 0, 1)
    forward(DOWN, 1, 1, 1)
    carry(0, 0, 2)
    forward_far(DOWN, 1, 0)
    diagonal(LATE)
    from_sibling(LATE)
    activate_late(0)
    forward_far(DOWN, 1, 1)
    token_begin(0, 2, DOWN)
    carry(0, 2, 3)
    token_begin(1, 1, UP)
    carry(0, 3, n_fo)
    settle(UP, 1)
    activate(1)

    @pl.when(ends)
    def _():
        weight_grad(DOWN, 1, 0)
        weight_grad(DOWN, 1, 1)

    carry(0, n_fo, 2 * n_fo + 2)
    activate_late(1)
    settle(DOWN, 1)
    token_partial(0, 2, DOWN)
    spread(0, 3)
    hidden_grad(1)
    carry(0, 2 * n_fo + 2, 2 * n_fo + 3)
    spread(0, 1)
    owned(DOWN, 0, 1)
    token_partial(1, 1, UP)

    @pl.when(jnp.logical_not(ends))
    def _():
        weight_grad(DOWN, 1, 0)
        weight_grad(DOWN, 1, 1)

    carry(0, 2 * n_fo + 3, 4 * n_fo + SKEW * (n_fo - 3))
    spread(1, 3)
    carry(1, 0, 1)
    spread(1, 1)
    spread(0, 2)
    carry(1, 1, 2)
    weight_grad(UP, 1, 0)
    spread(1, 2)
    weight_grad(UP, 1, 1)
    owned(UP, 0, 1)
    relay(0)
    carry(1, 2, 3)
    carry(1, 3, n_fo)
    carry(1, n_fo, 2 * n_fo)
    for w in (DOWN, UP):
        owned(w, 0, 0)
    relay(1)
    carry(1, 2 * n_fo, 2 * n_fo + 1)
    owned(DOWN, 1, 1)
    owned(DOWN, 1, 0)
    carry(1, 2 * n_fo + 1, 4 * n_fo + SKEW * (n_fo - 3))
    for w in (DOWN, UP):
        swapped(w, 0)
    owned(UP, 1, 1)
    collect(0)
    owned(UP, 1, 0)
    swapped(DOWN, 1)
    collect(1)
    swapped(UP, 1)

    for a in (COT, LATE):
        for j in range(8):
            token(a, j).wait_send()
    for w in range(2):
        for c in range(CHUNKS):
            across(w, c).wait_send()
            swap(w, c).wait_send()
        c = CHUNKS - 1
        for way in range(2):
            @pl.when(open_way(way))
            def _():
                for part in range(2):
                    along(w, c, fo, part, way).wait_send()

            for distance in range(1, n_fo):
                source, inside = incoming(way, distance)

                @pl.when(inside & open_way(way))
                def _():
                    for part in range(2):
                        along(w, c, source, part, way).wait_send()

            for block in range(n_fo):
                @pl.when(fo < block if way == 0 else fo > block)
                def _():
                    for part in range(2):
                        grad(w, c, block, part, way).wait_send()
    for a in range(2):
        for k in range(4):
            near(a, k).wait_send()
        for j in range(6):
            far(a, j).wait_send()


def layer(n_fo, n_tp, tokens, weights):
    rows, width = tokens[0].shape
    w_rows, cols = weights[0].shape
    wide = cols // 2 // CHUNKS
    count = 8 * rows
    dma = pltpu.SemaphoreType.DMA
    bf16, f32 = jnp.bfloat16, jnp.float32
    return pl.pallas_call(
        functools.partial(layer_kernel, n_fo, n_tp),
        out_shape=[jax.ShapeDtypeStruct((rows, width), bf16)] * 2
        + [jax.ShapeDtypeStruct((w_rows, cols), f32)] * 2,
        in_specs=[HBM] * 5,
        out_specs=[VMEM] * 4,
        scratch_shapes=[
            pltpu.VMEM((3, 2, 2, 2, rows, width), bf16),
            pltpu.VMEM((2, CHUNKS, n_fo, 2, w_rows, wide), bf16),
            pltpu.VMEM((2, CHUNKS, w_rows, wide), bf16),
            pltpu.VMEM((2, CHUNKS, n_fo, 2, w_rows, wide), bf16),
            pltpu.VMEM((2, 2, CHUNKS, n_fo, 2, w_rows, wide), bf16),
            pltpu.VMEM((count, wide), f32),
            pltpu.VMEM((3, CHUNKS, count, wide), bf16),
            pltpu.VMEM((2, 2, 2, 2, rows, width), bf16),
            pltpu.VMEM((2, 2, 2, rows, width), bf16),
            pltpu.VMEM((2, 2, 2, rows, width), bf16),
            pltpu.VMEM((2, 3, rows, width), bf16),
            pltpu.VMEM((2, CHUNKS, w_rows, wide), bf16),
            pltpu.VMEM((2, CHUNKS, w_rows, wide), bf16),
            dma((3 + 4 * CHUNKS,)), dma((2, 8)), dma((3, 8)), dma((2, CHUNKS)), dma((2, CHUNKS)),
            dma((2, n_fo + 1, 2)), dma((2, CHUNKS, n_fo, 2)),
            dma((2, 4)), dma((2, 4)), dma((2, 6)), dma((2, 6)),
            dma((2, n_fo, 2)), dma((2, CHUNKS, n_fo + 1, 2)),
            dma((2, CHUNKS)), dma((2, CHUNKS)),
        ],
        compiler_params=pltpu.CompilerParams(
            collective_id=0, has_side_effects=True, vmem_limit_bytes=50_000_000),
        name="layer",
    )(*(pltpu.with_memory_space_constraint(a, pltpu.HBM) for a in (*tokens, *weights)))


def finish_kernel(*refs):
    found, sums, results, (total, sems) = refs[0:4], refs[4:6], refs[6:10], refs[10:]
    copies = [pltpu.make_async_copy(found[a], results[a], sems.at[a]) for a in range(2)]
    for copy in copies:
        copy.start()
    for w in range(2):
        total[w] = sums[w][...] + found[2 + w][...]
        copies.append(pltpu.make_async_copy(total.at[w], results[2 + w], sems.at[2 + w]))
        copies[-1].start()
    for copy in copies:
        copy.wait()


def finish(found, sums):
    return pl.pallas_call(
        finish_kernel,
        out_shape=[jax.ShapeDtypeStruct(a.shape, a.dtype) for a in found],
        in_specs=[VMEM] * 6,
        out_specs=[pl.BlockSpec(memory_space=pl.ANY)] * 4,
        scratch_shapes=[pltpu.VMEM((2, *sums[0].shape), jnp.float32), pltpu.SemaphoreType.DMA((4,))],
        compiler_params=pltpu.CompilerParams(vmem_limit_bytes=8_000_000),
        name="finish",
    )(*found, *sums)


def on_device(n_fo, n_tp, x_late, x_early, cotangent, up_weight, down_weight, up_grad_sum, down_grad_sum):
    found = layer(n_fo, n_tp, (x_early, cotangent, x_late), (up_weight, down_weight))
    return tuple(finish(found, (up_grad_sum, down_grad_sum)))


def solution(mesh):
    n_fo, n_tp = mesh.shape["fs"] // 2, mesh.shape["tp"]
    assert n_tp == 4 and n_fo % 2 == 0
    rows, both = P(("fs", "tp"), None), P("fs", "tp")
    return jax.shard_map(
        functools.partial(on_device, n_fo, n_tp),
        mesh=mesh,
        in_specs=(rows, rows, rows, both, both, both, both),
        out_specs=(rows, rows, both, both),
        check_vma=False,
    )
```
